32 devices in a mesh: ep: 8 (over z, x), tp: 4 (over y, core).
Axes of the slice: x: 2, y: 2, z: 4, core: 2. Of those that a mesh axis runs over, the one named last changes fastest.
Arguments:
- glu_value: bfloat16 [32768, 1024], P(('ep', 'tp')), may hold values from -6 to 6
- glu_gate: bfloat16 [32768, 1024], P(('ep', 'tp')), may hold values from -6 to 6
- conv_taps: float32 [31, 1024], replicated, may hold values from -12 to 12
- chan_gain: float32 [1024], replicated, may hold values from 0.1 to 1.9
- chan_shift: float32 [1024], replicated, may hold values from -3 to 3
- mix_out_weight: bfloat16 [1024, 2048], P('tp'), may hold values from -0.1875 to 0.1875
- moe_input: bfloat16 [4096, 2048], P(('ep', 'tp')), may hold values from -6 to 6
- moe_gain: float32 [2048], replicated, may hold values from 0.1 to 1.9
- expert_ids: int32 [4096, 4], P(('ep', 'tp')), may hold values from 0 to 31, all different within a row; in each aligned block of 128 rows (0 to 127, 128 to 255, ...) at most 20 rows name the same one
- expert_share: float32 [4096, 4], P(('ep', 'tp')), may hold values from 0.05 to 1
- expert_gate_weight: bfloat16 [32, 2048, 1024], P(('ep', 'tp')), may hold values from -0.375 to 0.375
- expert_up_weight: bfloat16 [32, 2048, 1024], P(('ep', 'tp')), may hold values from -0.375 to 0.375
- expert_down_weight: bfloat16 [32, 1024, 2048], P(('ep', 'tp')), may hold values from -0.0390625 to 0.0390625
Outputs:
- mixed: bfloat16 [32768, 2048], P(('ep', 'tp'))
- moe_output: bfloat16 [4096, 2048], P(('ep', 'tp'))
The draws below stay inside these ranges and needn't reach their ends.
Inputs may be any that keep to these rules, and one draw needn't show every extreme that they name: `expert_ids`: each row names 4 different experts. In each aligned block of 128 rows (the rows of one device) no expert is named by more than 20 rows, and in some block one expert is named by exactly 20 rows.
All inputs are finite; a program needn't handle non-finite values.
Results may differ from the reference program's by a relative error of at most 0.0071.
Values may be sent and summed in bfloat16 or wider, within the bound.
A program may use at most 192 MiB of HBM per device.

```python
import math
import jax
import jax.numpy as jnp
import numpy as np
from jax import lax

D = 2048
CW = 1024
KERNEL = 31
FF = 1024
TOP = 4
MOE_TOK = 128
EXPERTS = 32
CAP = 20
MIX_LEN = 32768
MOE_LEN = 4096
N_EP = 8
N_TP = 4


def draw_conv_taps(key, part):
    base_key = jax.random.fold_in(key, 11)
    tap_key, chan_key = jax.random.split(base_key)
    chan_scale = jnp.exp(jax.random.uniform(chan_key, (1, CW), jnp.float32, 0.0, 2.3))
    tap_values = jax.random.truncated_normal(tap_key, -4.0, 4.0, (KERNEL, CW), jnp.float32)
    return (tap_values * chan_scale * KERNEL ** (-0.5)).astype(jnp.float32)


def block_scale(rng, dims, shards, low, top_value):
    def one(position, blocks):
        draws = jax.random.uniform(jax.random.fold_in(jax.random.fold_in(rng, 6), position), (blocks,), jnp.float32, low / len(shards), top_value / len(shards))
        return jnp.repeat(jnp.exp(draws), dims[position] // blocks).reshape((-1,) + (1,) * (len(dims) - position - 1))

    factor_of = one(*shards[0])
    for cut in shards[1:]:
        factor_of = factor_of * one(*cut)
    return factor_of


def shared_out(own_key, own, number, rows, count, top, reach, slope):
    order = jax.random.permutation(own_key, count)
    crowded, ordinary = portions_of(count, rows * top, reach, slope, True), portions_of(count, rows * top, reach, slope, False)
    places = jnp.arange(count)

    def named(lengths, offset_by):
        used = int((lengths > 0).sum())
        fixed = max(1, used // 4)
        shifted = fixed + (places - fixed + offset_by * (used - fixed)) % max(1, count - fixed)
        return jnp.zeros((count,), jnp.int32).at[order[jnp.where(places < fixed, places, shifted)]].set(jnp.asarray(lengths, jnp.int32))

    lengths = jnp.where(number % 4 == 0, named(crowded, number // 4), named(ordinary, number - number // 4 - 1))
    mixed = jax.random.permutation(jax.random.fold_in(own, 3), count)
    source_of, sink = mixed[0:count // 2 * 2:2], mixed[1:count // 2 * 2:2]
    slack = jnp.minimum(lengths[source_of] - 1, reach - lengths[sink]) // 2
    slack = jnp.where((source_of == order[0]) | (sink == order[0]) | (lengths[sink] == 0), 0, jnp.maximum(slack, 0))
    shifted = jax.random.randint(jax.random.fold_in(own, 4), (count // 2,), 0, 1 << 20) % (slack + 1)
    lengths = lengths.at[source_of].add(-shifted).at[sink].add(shifted)
    labels = jnp.searchsorted(jnp.cumsum(lengths), jnp.arange(rows * top), side="right").astype(jnp.int32)
    listing = labels.reshape(top, rows).T
    listing = listing[jax.random.permutation(jax.random.fold_in(own, 1), rows)]
    offset_by = jax.random.randint(jax.random.fold_in(own, 2), (rows, 1), 0, top)
    return jnp.take_along_axis(listing, (jnp.arange(top)[None, :] + offset_by) % top, axis=1)


def portions_of(amount, total, reach, skew, full):
    portions = [(1 << 20) // math.isqrt(rank ** skew) + 1 for rank in range(1, amount + 1)]
    largest = reach if full else min(reach, max(-(-total // amount), total * portions[0] // sum(portions)))
    least = 1 if total - largest >= amount - 1 else 0
    given, surplus = [largest] + [least] * (amount - 1), total - largest - least * (amount - 1)
    while surplus > 0:
        movable = [i for i in range(1, amount) if given[i] < largest] or [i for i in range(1, amount) if given[i] < reach]
        pool, budget = sum([portions[i] for i in movable]), surplus
        for i in movable:
            more = min(reach - given[i], max(1, budget * portions[i] // pool), surplus)
            given[i] = given[i] + more
            surplus = surplus - more
    return np.array(given)


def centred(stream_key, dims, deviation, reach, shards=(), kind=jnp.bfloat16):
    loudness = block_scale(stream_key, dims, shards, -0.22, 0.18) if shards else 1.0
    array = jax.random.normal(stream_key, dims, jnp.float32) * deviation * loudness
    return jnp.minimum(jnp.maximum(array, -reach), reach).astype(kind)


def setup_inputs(seed: int = 0) -> dict:
    seeds = jax.random.split(jax.random.key(seed), 14)
    glu_value = centred(seeds[0], (MIX_LEN, CW), 1.0, 6.0, ((0, 32),))
    glu_gate = centred(seeds[1], (MIX_LEN, CW), 1.0, 6.0, ((0, 32),))
    conv_taps = draw_conv_taps(jax.random.fold_in(seeds[13], 71), 0)
    chan_gain = jnp.clip(1.0 + 0.18 * jax.random.normal(seeds[3], (CW,), jnp.float32), 0.1, 1.9)
    chan_shift = centred(seeds[4], (CW,), 0.5, 3.0, (), jnp.float32)
    mix_out_weight = centred(seeds[5], (CW, D), CW ** -0.5, 0.1875, ((0, 4),))
    moe_input = centred(seeds[6], (MOE_LEN, D), 1.0, 6.0, ((0, 32),))
    moe_gain = jnp.clip(1.0 + 0.18 * jax.random.normal(seeds[7], (D,), jnp.float32), 0.1, 1.9)
    expert_ids_keys = jax.random.split(jax.random.fold_in(seeds[8], 1), MOE_LEN // MOE_TOK)
    expert_ids_turns = jax.random.permutation(jax.random.fold_in(seeds[8], 3), MOE_LEN // MOE_TOK)
    expert_ids = jax.vmap(lambda own, number: shared_out(jax.random.fold_in(seeds[8], 2), own, number, MOE_TOK, EXPERTS, TOP, CAP, 1))(expert_ids_keys, expert_ids_turns).reshape((MOE_LEN, TOP))
    expert_share = jnp.clip(jnp.exp(math.log(1.0) - 2.9957323 * jax.random.uniform(seeds[9], (MOE_LEN, TOP), jnp.float32) ** block_scale(seeds[9], (MOE_LEN, TOP), ((0, 32),), -0.2, 0.2)), 0.05, 1.0)
    expert_gate_weight = centred(seeds[10], (EXPERTS, D, FF), (D // 9) ** -0.5, 0.375, ((0, 32),))
    expert_up_weight = centred(seeds[11], (EXPERTS, D, FF), (D // 9) ** -0.5, 0.375, ((0, 32),))
    expert_down_weight = centred(seeds[12], (EXPERTS, FF, D), (25 * FF) ** -0.5, 0.0390625, ((0, 32),))
    return {"glu_value": glu_value, "glu_gate": glu_gate, "conv_taps": conv_taps, "chan_gain": chan_gain, "chan_shift": chan_shift, "mix_out_weight": mix_out_weight, "moe_input": moe_input, "moe_gain": moe_gain, "expert_ids": expert_ids, "expert_share": expert_share, "expert_gate_weight": expert_gate_weight, "expert_up_weight": expert_up_weight, "expert_down_weight": expert_down_weight}


CLAMP_LIMIT = 7.0
GLU_SLOPE = 1.702

def expert_apply(flat_rows, gate_matrix, up_matrix, down_matrix):
    pre_gate = jnp.dot(flat_rows, gate_matrix, preferred_element_type=jnp.float32)
    pre_up = jnp.dot(flat_rows, up_matrix, preferred_element_type=jnp.float32)
    gated = jnp.minimum(pre_gate, CLAMP_LIMIT)
    lifted = jnp.clip(pre_up, -CLAMP_LIMIT, CLAMP_LIMIT) + 1.0
    hidden = (lifted * gated * jax.nn.sigmoid(GLU_SLOPE * gated)).astype(jnp.bfloat16)
    return jnp.dot(hidden, down_matrix, preferred_element_type=jnp.float32).astype(jnp.bfloat16)

def reference(glu_value, glu_gate, conv_taps, chan_gain, chan_shift, mix_out_weight, moe_input, moe_gain, expert_ids, expert_share, expert_gate_weight, expert_up_weight, expert_down_weight):
    gated_input = glu_value.astype(jnp.float32) * jax.nn.sigmoid(glu_gate.astype(jnp.float32))
    padded = jnp.concatenate([jnp.zeros((KERNEL - 1, CW), jnp.float32), gated_input], 0)
    convolved = jnp.zeros((MIX_LEN, CW), jnp.float32)
    for offset in range(KERNEL):
        convolved = convolved + conv_taps[offset] * padded[offset:offset + MIX_LEN]
    center = lax.optimization_barrier(jnp.mean(convolved, axis=-1, keepdims=True))
    spread = lax.optimization_barrier(jnp.mean(jnp.square(convolved - center), axis=-1, keepdims=True))
    normalized = (convolved - center) * lax.rsqrt(spread + 1e-05) * chan_gain + chan_shift
    activated = jax.nn.silu(normalized).astype(jnp.bfloat16)
    mixed = jnp.dot(activated, mix_out_weight, preferred_element_type=jnp.float32).astype(jnp.bfloat16)
    features = moe_input.astype(jnp.float32)
    scaled = features * lax.rsqrt(lax.optimization_barrier(jnp.mean(jnp.square(features), axis=-1, keepdims=True)) + 1e-06)
    moe_normed = (scaled * moe_gain).astype(jnp.bfloat16)
    flat_ids = expert_ids.reshape(-1)
    flat_share = expert_share.reshape(-1)
    slots = N_EP * N_TP * CAP

    def one_expert(total, inputs):
        number, gate_matrix, up_matrix, down_matrix = inputs
        chosen = flat_ids == number
        picked = jnp.nonzero(chosen, size=slots, fill_value=0)[0].astype(jnp.int32)
        live = jnp.arange(slots, dtype=jnp.int32) < jnp.sum(chosen.astype(jnp.int32))
        token_rows = (picked // TOP).astype(jnp.int32)
        answers = expert_apply(moe_normed[token_rows], gate_matrix, up_matrix, down_matrix)
        weights = jnp.where(live, flat_share[picked], jnp.zeros((), flat_share.dtype))
        total = total.at[token_rows].add(weights[:, None] * answers.astype(jnp.float32))
        return (total, number)
    numbers = jnp.arange(EXPERTS, dtype=jnp.int32)
    total, unused = lax.scan(one_expert, jnp.zeros((MOE_LEN, D), jnp.float32), (numbers, expert_gate_weight, expert_up_weight, expert_down_weight))
    return (mixed, total.astype(jnp.bfloat16))
```

```python
import functools

import jax
import jax.numpy as jnp
from jax import lax
from jax.experimental import pallas as pl
from jax.experimental.pallas import tpu as pltpu
from jax.sharding import PartitionSpec as P

CLAMP_LIMIT = 7.0
GLU_SLOPE = 1.702
LANES = 128
PACK = 16
CUT = 2
KINDS = 4
MESH = pl.DeviceIdType.MESH
F32 = jnp.float32
BF16 = jnp.bfloat16


def place(flat, tp):
    return (flat // tp, flat % tp)


def rows_of(index, size):
    return pl.ds(pl.multiple_of(index * size, size), size)


def visit_order(depth):
    table = []
    for z in range(depth):
        near = sorted(range(depth), key=lambda other: (abs(other - z), other))
        table.append(near)
    return table


def source_at(depth, z, slot):
    table = visit_order(depth)
    picked = 0
    for a in range(depth):
        for b in range(depth):
            picked = picked + jnp.where((z == a) & (slot == b), table[a][b], 0)
    return picked


def remote(src, dst, ssem, rsem, flat, tp):
    return pltpu.make_async_remote_copy(
        src_ref=src,
        dst_ref=dst,
        send_sem=ssem,
        recv_sem=rsem,
        device_id=place(flat, tp),
        device_id_type=MESH,
    )


def greet(n, tp, slab, me, with_next):
    barrier = pltpu.get_barrier_semaphore()
    z, s = me // slab, me % slab
    depth = n // slab

    def hail(flat):
        pl.semaphore_signal(barrier, inc=1, device_id=place(flat, tp), device_id_type=MESH)

    @pl.loop(1, slab)
    def _(k):
        hail(z * slab + (s + k) % slab)

    edges = [(z < depth - 1, slab), (z > 0, -slab)]
    if with_next:
        edges.append(((s == slab - 1) & (z < depth - 1), 1))
        edges.append(((s == 0) & (z > 0), -1))
    total = slab - 1
    for there, step in edges:

        @pl.when(there)
        def _():
            hail(me + step)

        total = total + jnp.where(there, 1, 0)
    pl.semaphore_wait(barrier, total)


class Shape:
    def __init__(self, n, tp, tokens, per_token, width):
        slab = tp * max(1, tp // 2)
        while n % slab:
            slab //= 2
        self.n, self.tp, self.slab, self.depth = n, tp, slab, n // slab
        self.tokens, self.width = tokens, width
        copies = tokens * per_token
        capacity = max(2, 5 * copies // (4 * n))
        self.has_main = capacity >= PACK
        spare = 1
        while spare < capacity - PACK or (capacity < PACK and spare < capacity):
            spare *= 2
        self.spare = spare
        self.bits = spare.bit_length() - 1
        self.cuts = PACK // spare
        self.base = PACK if self.has_main else 0
        self.w = width // CUT
        self.main_w = self.w if self.has_main else 0
        self.piece = self.w // self.cuts
        self.block_w = self.main_w + self.piece
        self.pack_w = CUT * self.block_w
        self.slots = slab * PACK
        self.first = self.slots if self.has_main else 0
        self.count = self.first + slab * spare
        self.table_rows = -(-self.depth * KINDS // 8) * 8


def first_kernel(
    sh,
    taps_count,
    margin,
    tok,
    tab,
    value_all,
    gate_all,
    taps,
    gain,
    shift,
    weight,
    wg,
    wu,
    wd,
    answers,
    tabs_out,
    weight_out,
    act_out,
    held,
    tabs,
    packs,
    takes,
    data,
    hidden,
    total,
    reply,
    wg_v,
    wu_v,
    wd_v,
    value,
    gate,
    halo_v,
    halo_g,
    glu,
    conv,
    act,
    z_r,
    up_s,
    down_s,
    slab_s,
    slab_r,
    halo_s,
    halo_r,
    weight_s,
    weight_r,
    load_s,
    store_s,
):
    n, tp, slab, depth = sh.n, sh.tp, sh.slab, sh.depth
    e = lax.axis_index("ep")
    t = lax.axis_index("tp")
    me = e * tp + t
    z, s = me // slab, me % slab
    positions, channels = value.shape
    blocks = channels // LANES
    shard = weight.shape[0]
    chunk = shard // depth

    loads = [
        pltpu.make_async_copy(value_all, value, load_s.at[0]),
        pltpu.make_async_copy(gate_all, gate, load_s.at[1]),
        pltpu.make_async_copy(wg.at[0], wg_v, load_s.at[2]),
        pltpu.make_async_copy(wu.at[0], wu_v, load_s.at[3]),
        pltpu.make_async_copy(wd.at[0], wd_v, load_s.at[4]),
    ]
    for load in loads:
        load.start()

    def line_copy(part, src, own, up):
        if part < CUT:
            cols = slice(part * sh.w, (part + 1) * sh.w)
            there = held.at[src, :, cols]
            here = tok.at[:, cols] if own else there
        else:
            there = tabs.at[src]
            here = tab if own else there
        sems = up_s if up else down_s
        return remote(
            here, there, sems.at[src, part], z_r.at[src, part], me + (slab if up else -slab), tp
        )

    def halo_copy(which, dest):
        src, dst = ((value_all, halo_v), (gate_all, halo_g))[which]
        return remote(
            src.at[pl.ds(positions - margin, margin)],
            dst,
            halo_s.at[which],
            halo_r.at[which],
            dest,
            tp,
        )

    sibling = t + 1 - 2 * (t % 2)

    def weight_part(owner, c):
        start = pl.multiple_of(owner * shard + c * chunk, chunk)
        return weight_out.at[pl.ds(start, chunk)]

    def weight_copy(src, owner, c, dest, k):
        return remote(
            src, weight_part(owner, c), weight_s.at[k, c], weight_r.at[k, c], e * tp + dest, tp
        )

    def weight_own(c):
        return weight.at[rows_of(c, chunk)]

    def weight_far(k, owner, c):
        return weight_copy(weight_own(c), owner, c, (t + k) % tp, k)

    def weight_relay(k, c):
        owner = (t + tp - k) % tp
        return weight_copy(weight_part(owner, c), owner, c, sibling, k + 1)

    def weight_relayed(k, c):
        return weight_copy(weight_own(c), (sibling + tp - k) % tp, c, sibling, k + 1)

    def own_weight():
        return pltpu.make_async_copy(
            weight, weight_out.at[rows_of(t, shard)], store_s.at[0]
        )

    def block_copy(slot, h, k, sender, owner):
        cols = slice(h * sh.block_w, (h + 1) * sh.block_w)
        return remote(
            packs.at[slot, rows_of((s + k) % slab, PACK), cols],
            takes.at[slot, rows_of(sender, PACK), cols],
            slab_s.at[slot, h, k],
            slab_r.at[slot, h, k],
            z * slab + owner,
            tp,
        )

    def reply_copy(slot):
        return pltpu.make_async_copy(reply.at[slot], answers.at[slot], store_s.at[1 + slot])

    tile = positions // depth

    def act_copy(c):
        return pltpu.make_async_copy(
            act.at[rows_of(c, tile)], act_out.at[rows_of(c, tile)], store_s.at[1 + depth + c]
        )

    held[z] = tok[...]
    tabs[z] = tab[...]
    greet(n, tp, slab, me, True)

    for part in (CUT, *range(CUT)):

        @pl.when(z < depth - 1)
        def _():
            line_copy(part, z, True, True).start()

        @pl.when(z > 0)
        def _():
            line_copy(part, z, True, False).start()

    @pl.when(me < n - 1)
    def _():
        for which in range(2):
            halo_copy(which, me + 1).start()

    @pl.loop(0, depth)
    def _(c):
        weight_copy(weight_own(c), t, c, sibling, 1).start()

    own_weight().start()

    def pack_rows(slot, h, src):
        cols = h * sh.w
        token = lax.broadcasted_iota(jnp.int32, (sh.tokens, sh.slots), 0).astype(F32) + 1.0
        lane = lax.broadcasted_iota(jnp.int32, (sh.tokens, sh.slots), 1)
        at = h * sh.block_w

        def gathered(mask, lo, size):
            return lax.dot_general(
                mask.astype(F32).astype(BF16),
                held[src, :, lo : lo + size],
                (((0,), (0,)), ((), ())),
                preferred_element_type=F32,
            )

        if sh.has_main:
            named = tabs[src, pl.ds(z * KINDS, 1), :]
            packs[slot, :, at : at + sh.w] = gathered(named == token, cols, sh.w).astype(BF16)
        spare_named = tabs[src, pl.ds(z * KINDS + 2, 1), :]
        hit = spare_named == token
        part = (lane >> sh.bits) & (sh.cuts - 1)
        folded = jnp.zeros((sh.slots, sh.piece), F32)
        for q in range(sh.cuts):
            folded = folded + gathered(hit & (part == q), cols + q * sh.piece, sh.piece)
        packs[slot, :, at + sh.main_w : at + sh.block_w] = folded.astype(BF16)

    def home(shape, dim, q):
        row = lax.broadcasted_iota(jnp.int32, shape, dim)
        slot = lax.broadcasted_iota(jnp.int32, shape, 1 - dim)
        where = (row >> sh.bits) * PACK + (row & (sh.spare - 1)) + q * sh.spare
        return (where == slot).astype(F32).astype(BF16)

    spare_rows = slab * sh.spare
    hidden_units = wg_v.shape[1]
    block = min(256, hidden_units)

    def experts(slot):
        for h in range(CUT):
            at = h * sh.block_w
            if sh.has_main:
                data[0 : sh.slots, h * sh.w : (h + 1) * sh.w] = takes[slot, :, at : at + sh.w]
            rest = takes[slot, :, at + sh.main_w : at + sh.block_w]
            for q in range(sh.cuts):
                lo = h * sh.w + q * sh.piece
                data[sh.first : sh.count, lo : lo + sh.piece] = jnp.dot(
                    home((spare_rows, sh.slots), 0, q), rest, preferred_element_type=F32
                ).astype(BF16)

        for f in range(hidden_units // block):
            cols = slice(f * block, (f + 1) * block)
            pre_gate = jnp.dot(data[...], wg_v[:, cols], preferred_element_type=F32)
            pre_up = jnp.dot(data[...], wu_v[:, cols], preferred_element_type=F32)
            gated = jnp.minimum(pre_gate, CLAMP_LIMIT)
            lifted = jnp.clip(pre_up, -CLAMP_LIMIT, CLAMP_LIMIT) + 1.0
            hidden[:, cols] = (lifted * gated * jax.nn.sigmoid(GLU_SLOPE * gated)).astype(BF16)

        step = min(512, sh.width)
        for f in range(sh.width // step):
            cols = slice(f * step, (f + 1) * step)
            total[:, cols] = jnp.dot(
                hidden[...], wd_v[:, cols], preferred_element_type=F32
            ).astype(BF16)

        for h in range(CUT):
            at = h * sh.block_w
            if sh.has_main:
                reply[slot, :, at : at + sh.w] = total[0 : sh.slots, h * sh.w : (h + 1) * sh.w]
            folded = jnp.zeros((sh.slots, sh.piece), F32)
            for q in range(sh.cuts):
                lo = h * sh.w + q * sh.piece
                folded = folded + jnp.dot(
                    home((sh.slots, spare_rows), 1, q),
                    total[sh.first : sh.count, lo : lo + sh.piece],
                    preferred_element_type=F32,
                )
            reply[slot, :, at + sh.main_w : at + sh.block_w] = folded.astype(BF16)

    part = 64
    norm_part = 32
    lead = margin - (taps_count - 1)

    def conv_tile(c):
        top = c * tile
        for b in range(blocks):
            cols = slice(b * LANES, (b + 1) * LANES)
            here = rows_of(c, tile)
            there = pl.ds(pl.multiple_of(margin + top, PACK), tile)
            glu[b, there, :] = value[here, cols].astype(F32) * jax.nn.sigmoid(
                gate[here, cols].astype(F32)
            )

        @pl.loop(0, tile // part)
        def _(r):
            base = top + r * part
            for b in range(blocks):
                cols = slice(b * LANES, (b + 1) * LANES)
                summed = jnp.zeros((part, LANES), F32)
                for j in range(taps_count):
                    summed = (
                        summed + taps[j : j + 1, cols] * glu[b, pl.ds(base + lead + j, part), :]
                    )
                conv[rows_of(r, part), cols] = summed

        @pl.loop(0, tile // norm_part)
        def _(r):
            rows = conv[rows_of(r, norm_part), :]
            center = jnp.mean(rows, axis=-1, keepdims=True)
            rows = rows - center
            spread = jnp.mean(rows * rows, axis=-1, keepdims=True)
            normed = rows * lax.rsqrt(spread + 1e-05) * gain[...] + shift[...]
            there = pl.ds(pl.multiple_of(top + r * norm_part, norm_part), norm_part)
            act[there, :] = (normed * jax.nn.sigmoid(normed)).astype(BF16)

        act_copy(c).start()

    @pl.loop(0, depth + 1)
    def _(i):
        @pl.when(i < depth)
        def _():
            src = source_at(depth, z, i)
            for part in (CUT, *range(CUT)):

                @pl.when(i > 0)
                def _():
                    line_copy(part, src, False, True).wait_recv()

                @pl.when((i > 0) & (src < z) & (z < depth - 1))
                def _():
                    line_copy(part, src, False, True).start()

                @pl.when((src > z) & (z > 0))
                def _():
                    line_copy(part, src, False, False).start()

                if part < CUT:
                    pack_rows(i, part, src)

                    @pl.loop(1, slab)
                    def _(k):
                        block_copy(i, part, k, s, (s + k) % slab).start()

            takes[i, rows_of(s, PACK), :] = packs[i, rows_of(s, PACK), :]
            for k in range(2, tp, 2):
                weight_far(k, t, i).start()

        @pl.when(i > 0)
        def _():
            for k in range(2, tp, 2):
                weight_far(k, (t + tp - k) % tp, i - 1).wait_recv()
                weight_relay(k, i - 1).start()

        @pl.when(i == 0)
        def _():
            loads[0].wait()
            loads[1].wait()

            @pl.when(me > 0)
            def _():
                for which in range(2):
                    halo_copy(which, me - 1).wait_recv()
                for b in range(blocks):
                    cols = slice(b * LANES, (b + 1) * LANES)
                    glu[b, 0:margin, :] = halo_v[:, cols].astype(F32) * jax.nn.sigmoid(
                        halo_g[:, cols].astype(F32)
                    )

            @pl.when(me == 0)
            def _():
                for b in range(blocks):
                    glu[b, 0:margin, :] = jnp.zeros((margin, LANES), F32)

        low = jnp.where(i == 0, 0, jnp.minimum(i + 1, depth))
        high = jnp.minimum(i + 2, depth)

        @pl.loop(low, high)
        def _(c):
            conv_tile(c)

        @pl.when(i == 1)
        def _():
            for load in loads[2:]:
                load.wait()

        @pl.when(i > 0)
        def _():
            for h in range(CUT):

                @pl.loop(1, slab)
                def _(k):
                    block_copy(i - 1, h, k, (s + slab - k) % slab, s).wait_recv()

            experts(i - 1)
            reply_copy(i - 1).start()

    tabs_out[...] = tabs[...]

    @pl.when(me < n - 1)
    def _():
        for which in range(2):
            halo_copy(which, me + 1).wait_send()

    own_weight().wait()

    @pl.loop(0, depth)
    def _(c):
        weight_copy(weight_own(c), sibling, c, sibling, 1).wait_recv()
        weight_copy(weight_own(c), t, c, sibling, 1).wait_send()
        for k in range(2, tp, 2):
            weight_far(k, t, c).wait_send()
            weight_relayed(k, c).wait_recv()
            weight_relay(k, c).wait_send()
        act_copy(c).wait()
        reply_copy(c).wait()
        for part in range(CUT + 1):

            @pl.when((z < depth - 1) & (c <= z))
            def _():
                line_copy(part, c, False, True).wait_send()

            @pl.when((z > 0) & (c >= z))
            def _():
                line_copy(part, c, False, False).wait_send()

        for h in range(CUT):

            @pl.loop(1, slab)
            def _(k):
                block_copy(c, h, k, s, (s + k) % slab).wait_send()


def second_kernel(
    sh,
    answers,
    tabs,
    act,
    weight,
    moe_out,
    mixed,
    back,
    come,
    away,
    sums,
    act_v,
    weight_v,
    mixed_v,
    slab_s,
    slab_r,
    line_s,
    line_r,
    load_s,
    store_s,
):
    n, tp, slab, depth = sh.n, sh.tp, sh.slab, sh.depth
    me = lax.axis_index("ep") * tp + lax.axis_index("tp")
    z, s = me // slab, me % slab
    tiles = 2 * depth
    tile = act_v.shape[0] // tiles

    loads = [
        pltpu.make_async_copy(act, act_v, load_s.at[0]),
        pltpu.make_async_copy(weight, weight_v, load_s.at[1]),
    ]

    def block_copy(slot, h, k, owner, dest):
        cols = slice(h * sh.block_w, (h + 1) * sh.block_w)
        return remote(
            answers.at[slot, rows_of((s + k) % slab, PACK), cols],
            back.at[slot, rows_of(owner, PACK), cols],
            slab_s.at[slot, h, k],
            slab_r.at[slot, h, k],
            z * slab + dest,
            tp,
        )

    def own_copy(slot):
        return pltpu.make_async_copy(
            answers.at[slot, rows_of(s, PACK)], back.at[slot, rows_of(s, PACK)], load_s.at[2 + slot]
        )

    def line_copy(h, target, index, up):
        cols = slice(h * sh.w, (h + 1) * sh.w)
        return remote(
            away.at[target, :, cols],
            come.at[index, :, cols],
            line_s.at[target, h],
            line_r.at[index, h],
            me + (slab if up else -slab),
            tp,
        )

    def mixed_copy(c):
        return pltpu.make_async_copy(
            mixed_v.at[rows_of(c, tile)], mixed.at[rows_of(c, tile)], store_s.at[c]
        )

    greet(n, tp, slab, me, False)

    @pl.loop(0, depth)
    def _(m):
        slot = depth - 1 - m
        for h in range(CUT):

            @pl.loop(1, slab)
            def _(k):
                block_copy(slot, h, k, s, (s + k) % slab).start()

        own_copy(slot).start()

    for load in loads:
        load.start()
    for load in loads:
        load.wait()

    def weights_of(source, kind):
        token = lax.broadcasted_iota(jnp.int32, (sh.tokens, sh.slots), 0).astype(F32) + 1.0
        named = tabs[source, pl.ds(z * KINDS + kind, 1), :]
        share = tabs[source, pl.ds(z * KINDS + kind + 1, 1), :]
        full = jnp.where(named == token, share, 0.0)
        high = full.astype(BF16)
        low = (full - high.astype(F32)).astype(BF16)
        return high, low

    def weigh(high, low, rows):
        return jnp.dot(high, rows, preferred_element_type=F32) + jnp.dot(
            low, rows, preferred_element_type=F32
        )

    out_step = min(512, weight_v.shape[1])

    @pl.loop(0, depth)
    def _(m):
        slot = depth - 1 - m
        target = source_at(depth, z, slot)

        @pl.loop(0, 2)
        def _(u):
            c = m * 2 + u
            for f in range(weight_v.shape[1] // out_step):
                cols = slice(f * out_step, (f + 1) * out_step)
                mixed_v[rows_of(c, tile), cols] = jnp.dot(
                    act_v[rows_of(c, tile), :], weight_v[:, cols], preferred_element_type=F32
                ).astype(BF16)
            mixed_copy(c).start()

        own_copy(slot).wait()
        lane = lax.broadcasted_iota(jnp.int32, (sh.tokens, sh.slots), 1)
        part = (lane >> sh.bits) & (sh.cuts - 1)
        for h in range(CUT):

            @pl.loop(1, slab)
            def _(k):
                block_copy(slot, h, k, (s + slab - k) % slab, s).wait_recv()

            at = h * sh.block_w
            spare_high, spare_low = weights_of(target, 2)
            rest = back[slot, :, at + sh.main_w : at + sh.block_w]
            zero = jnp.zeros_like(spare_high)
            for q in range(sh.cuts):
                sums[:, q * sh.piece : (q + 1) * sh.piece] = weigh(
                    jnp.where(part == q, spare_high, zero),
                    jnp.where(part == q, spare_low, zero),
                    rest,
                )
            if sh.has_main:
                high, low = weights_of(target, 0)
                sums[...] += weigh(high, low, back[slot, :, at : at + sh.w])

            cols = slice(h * sh.w, (h + 1) * sh.w)
            from_below = (z > 0) & (target >= z)
            from_above = (z < depth - 1) & (target < z)
            final_above = (z < depth - 1) & (target == z)

            @pl.when(from_below | from_above)
            def _():
                line_copy(h, target, target, True).wait_recv()
                sums[...] += come[target, :, cols].astype(F32)

            @pl.when(final_above)
            def _():
                line_copy(h, target, depth, True).wait_recv()
                sums[...] += come[depth, :, cols].astype(F32)

            @pl.when(target == z)
            def _():
                moe_out[:, cols] = sums[...].astype(BF16)

            @pl.when(target != z)
            def _():
                away[target, :, cols] = sums[...].astype(BF16)

            @pl.when(target > z)
            def _():
                line_copy(h, target, target, True).start()

            @pl.when(target < z)
            def _():
                index = jnp.where(target == z - 1, depth, target)
                line_copy(h, target, index, False).start()

    @pl.loop(0, depth)
    def _(c):
        for h in range(CUT):

            @pl.loop(1, slab)
            def _(k):
                block_copy(c, h, k, s, (s + k) % slab).wait_send()

            @pl.when(c != z)
            def _():
                line_copy(h, c, c, True).wait_send()

    @pl.loop(0, tiles)
    def _(c):
        mixed_copy(c).wait()


ANY = pl.BlockSpec(memory_space=pl.ANY)
VMEM = pl.BlockSpec(memory_space=pltpu.VMEM)


def route_tables(sh, expert_ids, expert_share):
    n, tokens = sh.n, sh.tokens
    experts = jnp.arange(n, dtype=jnp.int32)
    chosen = (expert_ids[:, :, None] == experts).astype(F32)
    named = jnp.sum(chosen, axis=1).astype(BF16)
    below = (jnp.arange(tokens)[:, None] > jnp.arange(tokens)[None, :]).astype(BF16)
    before = jnp.dot(below, named, preferred_element_type=F32)
    rank = jnp.sum(before[:, None, :] * chosen, axis=2).astype(jnp.int32)

    lanes = jnp.arange(n * PACK, dtype=jnp.int32)
    main_code = jnp.where(rank < sh.base, expert_ids * PACK + rank, -1)
    spare_code = jnp.where(rank >= sh.base, expert_ids * sh.spare + rank - sh.base, -1)
    spare_lane = (lanes // PACK) * sh.spare + lanes % sh.spare
    number = jnp.arange(1, tokens + 1, dtype=jnp.int32).astype(F32)[:, None, None]
    share = expert_share[:, :, None]
    main_hit = main_code[:, :, None] == lanes
    spare_hit = spare_code[:, :, None] == spare_lane
    kinds = [
        jnp.sum(jnp.where(hit, what, 0.0), axis=(0, 1))
        for hit in (main_hit, spare_hit)
        for what in (number, share)
    ]
    table = jnp.stack([kind.reshape(sh.depth, sh.slots) for kind in kinds], axis=1)
    table = table.reshape(sh.depth * KINDS, sh.slots)
    return jnp.pad(table, ((0, sh.table_rows - sh.depth * KINDS), (0, 0)))


def body(
    n,
    tp,
    glu_value,
    glu_gate,
    conv_taps,
    chan_gain,
    chan_shift,
    mix_out_weight,
    moe_input,
    moe_gain,
    expert_ids,
    expert_share,
    expert_gate_weight,
    expert_up_weight,
    expert_down_weight,
):
    tokens, per_token = expert_ids.shape
    width = moe_input.shape[1]
    sh = Shape(n, tp, tokens, per_token, width)
    slab, depth = sh.slab, sh.depth

    features = moe_input.astype(F32)
    scaled = features * lax.rsqrt(jnp.mean(jnp.square(features), axis=-1, keepdims=True) + 1e-06)
    moe_normed = (scaled * moe_gain).astype(BF16)
    table = route_tables(sh, expert_ids, expert_share)

    positions, channels = glu_value.shape
    taps_count = conv_taps.shape[0]
    margin = -(-(taps_count - 1) // PACK) * PACK
    out_width = mix_out_weight.shape[1]
    hidden_units = expert_gate_weight.shape[2]
    dma = pltpu.SemaphoreType.DMA
    packed = (depth, sh.slots, sh.pack_w)
    answers, tabs, weight, act = pl.pallas_call(
        functools.partial(first_kernel, sh, taps_count, margin),
        name="dispatch_conv_experts",
        out_shape=(
            jax.ShapeDtypeStruct(packed, BF16),
            jax.ShapeDtypeStruct((depth, *table.shape), F32),
            jax.ShapeDtypeStruct((channels, out_width), BF16),
            jax.ShapeDtypeStruct((positions, channels), BF16),
        ),
        in_specs=[VMEM, VMEM, ANY, ANY, VMEM, VMEM, VMEM, VMEM, ANY, ANY, ANY],
        out_specs=(ANY, VMEM, ANY, ANY),
        scratch_shapes=[
            pltpu.VMEM((depth, tokens, width), BF16),
            pltpu.VMEM((depth, *table.shape), F32),
            pltpu.VMEM(packed, BF16),
            pltpu.VMEM(packed, BF16),
            pltpu.VMEM((sh.count, width), BF16),
            pltpu.VMEM((sh.count, hidden_units), BF16),
            pltpu.VMEM((sh.count, width), BF16),
            pltpu.VMEM(packed, BF16),
            pltpu.VMEM((width, hidden_units), BF16),
            pltpu.VMEM((width, hidden_units), BF16),
            pltpu.VMEM((hidden_units, width), BF16),
            pltpu.VMEM((positions, channels), BF16),
            pltpu.VMEM((positions, channels), BF16),
            pltpu.VMEM((margin, channels), BF16),
            pltpu.VMEM((margin, channels), BF16),
            pltpu.VMEM((channels // LANES, margin + positions, LANES), F32),
            pltpu.VMEM((positions // depth, channels), F32),
            pltpu.VMEM((positions, channels), BF16),
            dma((depth, CUT + 1)),
            dma((depth, CUT + 1)),
            dma((depth, CUT + 1)),
            dma((depth, CUT, slab)),
            dma((depth, CUT, slab)),
            dma((2,)),
            dma((2,)),
            dma((tp, depth)),
            dma((tp, depth)),
            dma((5,)),
            dma((1 + 2 * depth,)),
        ],
        compiler_params=pltpu.CompilerParams(
            collective_id=0, has_side_effects=True, vmem_limit_bytes=56 * 1024 * 1024
        ),
    )(
        moe_normed,
        table,
        glu_value,
        glu_gate,
        conv_taps,
        chan_gain.reshape(1, channels),
        chan_shift.reshape(1, channels),
        mix_out_weight,
        expert_gate_weight,
        expert_up_weight,
        expert_down_weight,
    )

    moe_output, mixed = pl.pallas_call(
        functools.partial(second_kernel, sh),
        name="return_and_mix",
        out_shape=(
            jax.ShapeDtypeStruct((tokens, width), BF16),
            jax.ShapeDtypeStruct((positions, out_width), BF16),
        ),
        in_specs=[ANY, VMEM, ANY, ANY],
        out_specs=(VMEM, ANY),
        scratch_shapes=[
            pltpu.VMEM(packed, BF16),
            pltpu.VMEM((depth + 1, tokens, width), BF16),
            pltpu.VMEM((depth, tokens, width), BF16),
            pltpu.VMEM((tokens, sh.w), F32),
            pltpu.VMEM((positions, channels), BF16),
            pltpu.VMEM((channels, out_width), BF16),
            pltpu.VMEM((positions, out_width), BF16),
            dma((depth, CUT, slab)),
            dma((depth, CUT, slab)),
            dma((depth, CUT)),
            dma((depth + 1, CUT)),
            dma((2 + depth,)),
            dma((2 * depth,)),
        ],
        compiler_params=pltpu.CompilerParams(
            collective_id=1, has_side_effects=True, vmem_limit_bytes=48 * 1024 * 1024
        ),
    )(answers, tabs, act, weight)
    return (mixed, moe_output)


def solution(mesh):
    tp = mesh.shape["tp"]
    n = mesh.shape["ep"] * tp
    both = P(("ep", "tp"), None)
    weights = P(("ep", "tp"), None, None)
    placed = (
        both, both, P(), P(), P(), P("tp", None), both, P(), both, both, weights, weights, weights
    )
    return jax.shard_map(
        functools.partial(body, n, tp),
        mesh=mesh,
        in_specs=placed,
        out_specs=(both, both),
        check_vma=False,
    )
```

```python
import functools

import jax
import jax.numpy as jnp
from jax import lax
from jax.experimental import pallas as pl
from jax.experimental.pallas import tpu as pltpu
from jax.sharding import PartitionSpec as P

CLAMP_LIMIT = 7.0
GLU_SLOPE = 1.702
LANES = 128
PACK = 16
CUT = 2
HOP = 4
KINDS = 4
FEED = 2
MESH = pl.DeviceIdType.MESH
F32 = jnp.float32
BF16 = jnp.bfloat16


def place(flat, tp):
    return (flat // tp, flat % tp)


def rows_of(index, size):
    return pl.ds(pl.multiple_of(index * size, size), size)


def visit_order(depth):
    table = []
    for z in range(depth):
        near = sorted(range(depth), key=lambda other: (abs(other - z), other))
        table.append(near)
    return table


def drain_order(depth):
    table = []
    for z in range(depth):
        upward = [(z + k, z + k) for k in range(1, depth - z)] if z > 0 else []
        downward = (
            [(depth - 1 - z + k, z - k) for k in range(1, z + 1)] if z < depth - 1 else []
        )
        events = [target for _, target in sorted(upward + downward)]
        table.append(events + [-1] * (depth - len(events)))
    return table


def looked_up(table, z, slot):
    picked = 0
    for a, row in enumerate(table):
        for b, entry in enumerate(row):
            picked = picked + jnp.where((z == a) & (slot == b), entry, 0)
    return picked


def remote(src, dst, ssem, rsem, flat, tp):
    return pltpu.make_async_remote_copy(
        src_ref=src,
        dst_ref=dst,
        send_sem=ssem,
        recv_sem=rsem,
        device_id=place(flat, tp),
        device_id_type=MESH,
    )


def greet(n, tp, slab, me, with_next):
    barrier = pltpu.get_barrier_semaphore()
    z, s = me // slab, me % slab
    depth = n // slab

    def hail(flat):
        pl.semaphore_signal(barrier, inc=1, device_id=place(flat, tp), device_id_type=MESH)

    @pl.loop(1, slab)
    def _(k):
        hail(z * slab + (s + k) % slab)

    edges = [(z < depth - 1, slab), (z > 0, -slab)]
    if with_next:
        edges.append(((s == slab - 1) & (z < depth - 1), 1))
        edges.append(((s == 0) & (z > 0), -1))
    total = slab - 1
    for there, step in edges:

        @pl.when(there)
        def _():
            hail(me + step)

        total = total + jnp.where(there, 1, 0)
    return total


class Shape:
    def __init__(self, n, tp, tokens, per_token, width):
        slab = tp * max(1, tp // 2)
        while n % slab:
            slab //= 2
        self.n, self.tp, self.slab, self.depth = n, tp, slab, n // slab
        self.tokens, self.width = tokens, width
        copies = tokens * per_token
        capacity = max(2, 5 * copies // (4 * n))
        self.has_main = capacity >= PACK
        spare = 1
        while spare < capacity - PACK or (capacity < PACK and spare < capacity):
            spare *= 2
        self.spare = spare
        self.bits = spare.bit_length() - 1
        self.cuts = PACK // spare
        self.base = PACK if self.has_main else 0
        self.w = width // CUT
        self.main_w = self.w if self.has_main else 0
        self.piece = self.w // self.cuts
        self.block_w = self.main_w + self.piece
        self.pack_w = CUT * self.block_w
        self.slots = slab * PACK
        self.first = self.slots if self.has_main else 0
        self.count = self.first + slab * spare
        self.table_rows = -(-self.depth * KINDS // 8) * 8


def prepare(sh, features_ref, gain, id_rows, share_rows, normed, table):
    n, tokens = sh.n, sh.tokens
    features = features_ref[...].astype(F32)
    scale = lax.rsqrt(jnp.mean(features * features, axis=-1, keepdims=True) + 1e-06)
    normed[...] = (features * scale * gain[...]).astype(BF16)

    def upright(rows):
        rows = rows[...].astype(F32)
        blank = jnp.zeros((8 - rows.shape[0] % 8, tokens), F32)
        return jnp.transpose(jnp.concatenate([rows, blank], axis=0))

    ids = upright(id_rows).astype(jnp.int32)
    share = upright(share_rows)
    expert = lax.broadcasted_iota(jnp.int32, (tokens, n), 1)
    hits = [(ids[:, k : k + 1] == expert).astype(F32) for k in range(id_rows.shape[0])]
    named = hits[0]
    for hit in hits[1:]:
        named = named + hit
    below = (
        lax.broadcasted_iota(jnp.int32, (tokens, tokens), 0)
        > lax.broadcasted_iota(jnp.int32, (tokens, tokens), 1)
    )
    before = jnp.dot(
        below.astype(F32).astype(BF16), named.astype(BF16), preferred_element_type=F32
    )
    number = lax.broadcasted_iota(jnp.int32, (tokens, sh.slots), 0).astype(F32) + 1.0
    lane = lax.broadcasted_iota(jnp.int32, (tokens, sh.slots), 1)
    main_lane = lane
    spare_lane = lane // PACK * sh.spare + lane % sh.spare
    codes = []
    for k, hit in enumerate(hits):
        chosen = ids[:, k : k + 1]
        rank = jnp.sum(before * hit, axis=1, keepdims=True).astype(jnp.int32)
        main_code = jnp.where(rank < sh.base, chosen * PACK + rank, -1)
        spare_code = jnp.where(rank >= sh.base, chosen * sh.spare + rank - sh.base, -1)
        codes.append((main_code, spare_code, share[:, k : k + 1]))
    table[...] = jnp.zeros_like(table)
    for z in range(sh.depth):
        for kind, lanes, start in (
            (0, main_lane, z * sh.slots),
            (1, spare_lane, z * sh.slab * sh.spare),
        ):
            names = jnp.zeros((tokens, sh.slots), F32)
            shares = jnp.zeros((tokens, sh.slots), F32)
            for code in codes:
                hit = code[kind] - start == lanes
                names = names + jnp.where(hit, number, 0.0)
                shares = shares + jnp.where(hit, code[2], 0.0)
            row = z * KINDS + 2 * kind
            table[row : row + 1, :] = jnp.sum(names, axis=0, keepdims=True)
            table[row + 1 : row + 2, :] = jnp.sum(shares, axis=0, keepdims=True)


def whole_kernel(
    sh,
    taps_count,
    margin,
    moe,
    moe_gain,
    id_rows,
    share_rows,
    value_all,
    gate_all,
    taps,
    gain,
    shift,
    weight,
    wg,
    wu,
    wd,
    mixed,
    moe_out,
    held,
    tabs,
    packs,
    takes,
    data,
    hidden,
    total,
    reply,
    back,
    come,
    away,
    parts,
    wg_v,
    wu_v,
    wd_v,
    weight_v,
    value,
    gate,
    halo_v,
    halo_g,
    glu,
    conv,
    act,
    z_r,
    up_s,
    down_s,
    slab_s,
    slab_r,
    back_s,
    back_r,
    line_s,
    line_r,
    halo_s,
    halo_r,
    weight_s,
    weight_r,
    cross_s,
    cross_r,
    load_s,
    moe_v,
    moe_gain_v,
    id_v,
    share_v,
    taps_v,
    gain_v,
    shift_v,
):
    n, tp, slab, depth = sh.n, sh.tp, sh.slab, sh.depth
    e = lax.axis_index("ep")
    t = lax.axis_index("tp")
    me = e * tp + t
    z, s = me // slab, me % slab
    positions, channels = value.shape
    blocks = channels // LANES
    shard = weight.shape[0]
    order = visit_order(depth)
    late = drain_order(depth)

    loads = [
        pltpu.make_async_copy(value_all, value, load_s.at[0]),
        pltpu.make_async_copy(gate_all, gate, load_s.at[1]),
        pltpu.make_async_copy(wg.at[0], wg_v, load_s.at[2]),
        pltpu.make_async_copy(wu.at[0], wu_v, load_s.at[3]),
        pltpu.make_async_copy(wd.at[0], wd_v, load_s.at[4]),
        pltpu.make_async_copy(weight, weight_v.at[rows_of(t, shard)], load_s.at[5]),
    ]
    small = [
        pltpu.make_async_copy(here, there, load_s.at[6 + at])
        for at, (here, there) in enumerate(
            (
                (moe, moe_v),
                (moe_gain, moe_gain_v),
                (id_rows, id_v),
                (share_rows, share_v),
                (taps, taps_v),
                (gain, gain_v),
                (shift, shift_v),
            )
        )
    ]
    for load in small + loads:
        load.start()

    def line_copy(part, src, up):
        if part < CUT:
            cols = slice(part * sh.w, (part + 1) * sh.w)
            there = held.at[src, :, cols]
            here = there
        else:
            there = tabs.at[src]
            here = there
        sems = up_s if up else down_s
        return remote(
            here, there, sems.at[src, part], z_r.at[src, part], me + (slab if up else -slab), tp
        )

    def halo_copy(which, dest):
        src, dst = ((value_all, halo_v), (gate_all, halo_g))[which]
        return remote(
            src.at[pl.ds(positions - margin, margin)],
            dst,
            halo_s.at[which],
            halo_r.at[which],
            dest,
            tp,
        )

    sibling = t + 1 - 2 * (t % 2)
    across = slab // tp
    halves = 2 if across % 2 == 0 else 1
    x = (me // tp) % across
    mine = x % halves
    partner = e + 1 - 2 * (x % 2)
    chunk = shard // (halves * FEED)

    def weight_rows(owner, half, c):
        start = owner * shard + (half * FEED + c) * chunk
        return weight_v.at[pl.ds(pl.multiple_of(start, chunk), chunk)]

    def weight_far(k, owner, c):
        start = pl.multiple_of((mine * FEED + c) * chunk, chunk)
        return remote(
            weight.at[pl.ds(start, chunk)],
            weight_rows(owner, mine, c),
            weight_s.at[k, c],
            weight_r.at[k, c],
            e * tp + (t + k) % tp,
            tp,
        )

    def weight_relay(k, owner, c):
        here = weight_rows(owner, mine, c)
        return remote(
            here, here, weight_s.at[k + 1, c], weight_r.at[k + 1, c], e * tp + sibling, tp
        )

    def weight_cross(k, owner, half, c):
        here = weight_rows(owner, half, c)
        return remote(here, here, cross_s.at[k, c], cross_r.at[k, c], partner * tp + t, tp)

    def cross_relay(k, owner, c):
        here = weight_rows(owner, 1 - mine, c)
        return remote(here, here, cross_s.at[k + 1, c], cross_r.at[k + 1, c], e * tp + sibling, tp)

    def weight_own(owner):
        return remote(
            weight,
            weight_v.at[rows_of(owner, shard)],
            weight_s.at[1, 0],
            weight_r.at[1, 0],
            e * tp + sibling,
            tp,
        )

    def far_owner(base, k):
        return (base + tp - k) % tp

    def block_copy(slot, h, k, sender, owner):
        cols = slice(h * sh.block_w, (h + 1) * sh.block_w)
        return remote(
            packs.at[slot, rows_of((s + k) % slab, PACK), cols],
            takes.at[slot, rows_of(sender, PACK), cols],
            slab_s.at[slot, h, k],
            slab_r.at[slot, h, k],
            z * slab + owner,
            tp,
        )

    def back_copy(slot, h, k, owner, dest):
        cols = slice(h * sh.block_w, (h + 1) * sh.block_w)
        return remote(
            reply.at[slot, rows_of((s + k) % slab, PACK), cols],
            back.at[slot, rows_of(owner, PACK), cols],
            back_s.at[slot, h, k],
            back_r.at[slot, h, k],
            z * slab + dest,
            tp,
        )

    hop_w = sh.width // HOP
    fold = HOP // CUT

    def chain_copy(p, target, index, up):
        cols = slice(p * hop_w, (p + 1) * hop_w)
        return remote(
            away.at[target, :, cols],
            come.at[index, :, cols],
            line_s.at[target, p],
            line_r.at[index, p],
            me + (slab if up else -slab),
            tp,
        )

    expected = greet(n, tp, slab, me, True)
    for load in small:
        load.wait()
    prepare(sh, moe_v, moe_gain_v, id_v, share_v, held.at[z], tabs.at[z])
    pl.semaphore_wait(pltpu.get_barrier_semaphore(), expected)

    for part in (CUT, *range(CUT)):

        @pl.when(z < depth - 1)
        def _():
            line_copy(part, z, True).start()

        @pl.when(z > 0)
        def _():
            line_copy(part, z, False).start()

    @pl.when(me < n - 1)
    def _():
        for which in range(2):
            halo_copy(which, me + 1).start()

    weight_own(t).start()

    def arrive(k, part):
        for src, there, onward, up in (
            (z - k, z >= k, z < depth - 1, True),
            (z + k, z + k < depth, z > 0, False),
        ):

            @pl.when(there)
            def _():
                line_copy(part, src, up).wait_recv()

            @pl.when(there & onward)
            def _():
                line_copy(part, src, up).start()

    def pack_rows(slot, h, src):
        cols = h * sh.w
        token = lax.broadcasted_iota(jnp.int32, (sh.tokens, sh.slots), 0).astype(F32) + 1.0
        lane = lax.broadcasted_iota(jnp.int32, (sh.tokens, sh.slots), 1)
        at = h * sh.block_w

        def gathered(mask, lo, size):
            return lax.dot_general(
                mask.astype(F32).astype(BF16),
                held[src, :, lo : lo + size],
                (((0,), (0,)), ((), ())),
                preferred_element_type=F32,
            )

        if sh.has_main:
            named = tabs[src, pl.ds(z * KINDS, 1), :]
            packs[slot, :, at : at + sh.w] = gathered(named == token, cols, sh.w).astype(BF16)
        spare_named = tabs[src, pl.ds(z * KINDS + 2, 1), :]
        hit = spare_named == token
        part = (lane >> sh.bits) & (sh.cuts - 1)
        folded = jnp.zeros((sh.slots, sh.piece), F32)
        for q in range(sh.cuts):
            folded = folded + gathered(hit & (part == q), cols + q * sh.piece, sh.piece)
        packs[slot, :, at + sh.main_w : at + sh.block_w] = folded.astype(BF16)

    def home(shape, dim, q):
        row = lax.broadcasted_iota(jnp.int32, shape, dim)
        slot = lax.broadcasted_iota(jnp.int32, shape, 1 - dim)
        where = (row >> sh.bits) * PACK + (row & (sh.spare - 1)) + q * sh.spare
        return (where == slot).astype(F32).astype(BF16)

    spare_rows = slab * sh.spare
    hidden_units = wg_v.shape[1]
    block = min(256, hidden_units)

    def experts(slot):
        for h in range(CUT):
            at = h * sh.block_w
            if sh.has_main:
                data[0 : sh.slots, h * sh.w : (h + 1) * sh.w] = takes[slot, :, at : at + sh.w]
            rest = takes[slot, :, at + sh.main_w : at + sh.block_w]
            for q in range(sh.cuts):
                lo = h * sh.w + q * sh.piece
                data[sh.first : sh.count, lo : lo + sh.piece] = jnp.dot(
                    home((spare_rows, sh.slots), 0, q), rest, preferred_element_type=F32
                ).astype(BF16)

        for f in range(hidden_units // block):
            cols = slice(f * block, (f + 1) * block)
            pre_gate = jnp.dot(data[...], wg_v[:, cols], preferred_element_type=F32)
            pre_up = jnp.dot(data[...], wu_v[:, cols], preferred_element_type=F32)
            gated = jnp.minimum(pre_gate, CLAMP_LIMIT)
            lifted = jnp.clip(pre_up, -CLAMP_LIMIT, CLAMP_LIMIT) + 1.0
            hidden[:, cols] = (lifted * gated * jax.nn.sigmoid(GLU_SLOPE * gated)).astype(BF16)

        step = min(512, sh.width)
        for f in range(sh.width // step):
            cols = slice(f * step, (f + 1) * step)
            total[:, cols] = jnp.dot(
                hidden[...], wd_v[:, cols], preferred_element_type=F32
            ).astype(BF16)

        for h in range(CUT):
            at = h * sh.block_w
            if sh.has_main:
                reply[slot, :, at : at + sh.w] = total[0 : sh.slots, h * sh.w : (h + 1) * sh.w]
            folded = jnp.zeros((sh.slots, sh.piece), F32)
            for q in range(sh.cuts):
                lo = h * sh.w + q * sh.piece
                folded = folded + jnp.dot(
                    home((sh.slots, spare_rows), 1, q),
                    total[sh.first : sh.count, lo : lo + sh.piece],
                    preferred_element_type=F32,
                )
            reply[slot, :, at + sh.main_w : at + sh.block_w] = folded.astype(BF16)

    part_rows = 64
    norm_rows = 32
    lead = margin - (taps_count - 1)
    tile = positions // depth

    def conv_tile(c):
        top = c * tile
        here = rows_of(c, tile)

        @pl.when(c > 0)
        def _():
            for b in range(blocks):
                glu[b, 0:margin, :] = glu[b, tile : tile + margin, :]

        for b in range(blocks):
            cols = slice(b * LANES, (b + 1) * LANES)
            glu[b, margin : margin + tile, :] = value[here, cols].astype(F32) * jax.nn.sigmoid(
                gate[here, cols].astype(F32)
            )

        @pl.loop(0, tile // part_rows)
        def _(r):
            base = r * part_rows
            for b in range(blocks):
                cols = slice(b * LANES, (b + 1) * LANES)
                summed = jnp.zeros((part_rows, LANES), F32)
                for j in range(taps_count):
                    summed = (
                        summed
                        + taps_v[j : j + 1, cols] * glu[b, pl.ds(base + lead + j, part_rows), :]
                    )
                conv[rows_of(r, part_rows), cols] = summed

        @pl.loop(0, tile // norm_rows)
        def _(r):
            rows = conv[rows_of(r, norm_rows), :]
            center = jnp.mean(rows, axis=-1, keepdims=True)
            rows = rows - center
            spread = jnp.mean(rows * rows, axis=-1, keepdims=True)
            normed = rows * lax.rsqrt(spread + 1e-05) * gain_v[...] + shift_v[...]
            there = pl.ds(pl.multiple_of(top + r * norm_rows, norm_rows), norm_rows)
            act[there, :] = (normed * jax.nn.sigmoid(normed)).astype(BF16)

    def weights_of(source, kind):
        token = lax.broadcasted_iota(jnp.int32, (sh.tokens, sh.slots), 0).astype(F32) + 1.0
        named = tabs[source, pl.ds(z * KINDS + kind, 1), :]
        share = tabs[source, pl.ds(z * KINDS + kind + 1, 1), :]
        full = jnp.where(named == token, share, 0.0)
        high = full.astype(BF16)
        low = (full - high.astype(F32)).astype(BF16)
        return high, low

    def weigh(high, low, rows):
        return jnp.dot(high, rows, preferred_element_type=F32) + jnp.dot(
            low, rows, preferred_element_type=F32
        )

    def pass_on(p, target):
        @pl.when(target > z)
        def _():
            chain_copy(p, target, target, True).start()

        @pl.when(target < z)
        def _():
            index = jnp.where(target == z - 1, depth, target)
            chain_copy(p, target, index, False).start()

    def combine(slot):
        target = looked_up(order, z, slot)
        begins = ((z == 0) & (target > 0)) | ((z == depth - 1) & (target < z))
        lane = lax.broadcasted_iota(jnp.int32, (sh.tokens, sh.slots), 1)
        part = (lane >> sh.bits) & (sh.cuts - 1)
        for h in range(CUT):

            @pl.loop(1, slab)
            def _(k):
                back_copy(slot, h, k, (s + slab - k) % slab, s).wait_recv()

            at = h * sh.block_w
            cols = slice(h * sh.w, (h + 1) * sh.w)
            spare_high, spare_low = weights_of(target, 2)
            rest = back[slot, :, at + sh.main_w : at + sh.block_w]
            zero = jnp.zeros_like(spare_high)
            for q in range(sh.cuts):
                lo = h * sh.w + q * sh.piece
                parts[target, :, lo : lo + sh.piece] = weigh(
                    jnp.where(part == q, spare_high, zero),
                    jnp.where(part == q, spare_low, zero),
                    rest,
                )
            if sh.has_main:
                high, low = weights_of(target, 0)
                parts[target, :, cols] += weigh(high, low, back[slot, :, at : at + sh.w])

            @pl.when(begins)
            def _():
                away[target, :, cols] = parts[target, :, cols].astype(BF16)
                for f in range(fold):
                    pass_on(h * fold + f, target)

    out_w = weight_v.shape[1]
    out_step = min(512, out_w)
    mix_rows = positions // (2 * depth)

    def mix(c):
        for f in range(out_w // out_step):
            cols = slice(f * out_step, (f + 1) * out_step)
            mixed[rows_of(c, mix_rows), cols] = jnp.dot(
                act[rows_of(c, mix_rows), :], weight_v[:, cols], preferred_element_type=F32
            ).astype(BF16)

    def dispatch(slot, h):
        pack_rows(slot, h, looked_up(order, z, slot))

        @pl.loop(1, slab)
        def _(k):
            block_copy(slot, h, k, s, (s + k) % slab).start()

        cols = slice(h * sh.block_w, (h + 1) * sh.block_w)
        takes[slot, rows_of(s, PACK), cols] = packs[slot, rows_of(s, PACK), cols]

    def send_back(slot):
        for h in range(CUT):

            @pl.loop(1, slab)
            def _(k):
                back_copy(slot, h, k, s, (s + k) % slab).start()

        back[slot, rows_of(s, PACK), :] = reply[slot, rows_of(s, PACK), :]

    last = CUT - 1

    @pl.loop(0, depth + 3)
    def _(i):
        @pl.when(i == depth + 2)
        def _():
            @pl.loop(0, depth)
            def _(k):
                target = looked_up(late, z, k)

                @pl.when(target >= 0)
                def _():
                    for p in range(HOP):
                        cols = slice(p * hop_w, (p + 1) * hop_w)
                        chain_copy(p, target, target, True).wait_recv()
                        away[target, :, cols] = (
                            parts[target, :, cols] + come[target, :, cols].astype(F32)
                        ).astype(BF16)
                        pass_on(p, target)

        @pl.when(i > 2)
        def _():
            combine((i - 2) % depth)

        @pl.when((i > 0) & (i < depth))
        def _():
            arrive(i, last)

        @pl.when(i < depth)
        def _():
            for h in range(last):

                @pl.when(i == 0)
                def _():
                    dispatch(i, h)

            dispatch(i, last)

        for k in range(2, tp, 2):

            @pl.when(i < FEED)
            def _():
                weight_far(k, t, i).start()

            @pl.when((i > 0) & (i <= FEED))
            def _():
                weight_far(k, far_owner(t, k), i - 1).wait_recv()
                weight_relay(k, far_owner(t, k), i - 1).start()
                if halves == 2:
                    weight_cross(k, far_owner(t, k), mine, i - 1).start()

            if halves == 2:

                @pl.when((i > 1) & (i <= FEED + 1))
                def _():
                    weight_cross(k, far_owner(t, k), 1 - mine, i - 2).wait_recv()
                    cross_relay(k, far_owner(t, k), i - 2).start()

        @pl.when(i == 0)
        def _():
            loads[0].wait()
            loads[1].wait()

            @pl.when(me > 0)
            def _():
                for which in range(2):
                    halo_copy(which, me - 1).wait_recv()
                for b in range(blocks):
                    cols = slice(b * LANES, (b + 1) * LANES)
                    glu[b, 0:margin, :] = halo_v[:, cols].astype(F32) * jax.nn.sigmoid(
                        halo_g[:, cols].astype(F32)
                    )

            @pl.when(me == 0)
            def _():
                for b in range(blocks):
                    glu[b, 0:margin, :] = jnp.zeros((margin, LANES), F32)

        @pl.when(i < depth)
        def _():
            conv_tile(i)

        @pl.when(i < depth - 1)
        def _():
            arrive(i + 1, CUT)
            for h in range(last):
                arrive(i + 1, h)
                dispatch(i + 1, h)

        @pl.when(i == 0)
        def _():
            for load in loads[2:]:
                load.wait()

        @pl.when(i < depth)
        def _():
            for h in range(CUT):

                @pl.loop(1, slab)
                def _(k):
                    block_copy(i, h, k, (s + slab - k) % slab, s).wait_recv()

            experts(i)

        @pl.when((i > 0) & (i <= depth))
        def _():
            send_back(i % depth)

        @pl.when(i == depth)
        def _():
            weight_own(sibling).wait_recv()

            @pl.loop(0, FEED)
            def _(c):
                for k in range(2, tp, 2):
                    weight_relay(k, far_owner(sibling, k), c).wait_recv()
                    if halves == 2:
                        cross_relay(k, far_owner(sibling, k), c).wait_recv()

            @pl.loop(0, 2 * depth)
            def _(c):
                mix(c)

    for p in range(HOP):
        cols = slice(p * hop_w, (p + 1) * hop_w)

        @pl.when(z > 0)
        def _():
            chain_copy(p, z, z, True).wait_recv()
            parts[z, :, cols] += come[z, :, cols].astype(F32)

        @pl.when(z < depth - 1)
        def _():
            chain_copy(p, z, depth, True).wait_recv()
            parts[z, :, cols] += come[depth, :, cols].astype(F32)

        moe_out[:, cols] = parts[z, :, cols].astype(BF16)

    @pl.when(me < n - 1)
    def _():
        for which in range(2):
            halo_copy(which, me + 1).wait_send()

    weight_own(t).wait_send()

    @pl.loop(0, FEED)
    def _(c):
        for k in range(2, tp, 2):
            weight_far(k, t, c).wait_send()
            weight_relay(k, far_owner(t, k), c).wait_send()
            if halves == 2:
                weight_cross(k, far_owner(t, k), mine, c).wait_send()
                cross_relay(k, far_owner(t, k), c).wait_send()

    @pl.loop(0, depth)
    def _(c):
        for part in range(CUT + 1):

            @pl.when((z < depth - 1) & (c <= z))
            def _():
                line_copy(part, c, True).wait_send()

            @pl.when((z > 0) & (c >= z))
            def _():
                line_copy(part, c, False).wait_send()

        for h in range(CUT):

            @pl.loop(1, slab)
            def _(k):
                block_copy(c, h, k, s, (s + k) % slab).wait_send()
                back_copy(c, h, k, s, (s + k) % slab).wait_send()

        @pl.when(c != z)
        def _():
            for p in range(HOP):
                chain_copy(p, c, c, True).wait_send()


ANY = pl.BlockSpec(memory_space=pl.ANY)
VMEM = pl.BlockSpec(memory_space=pltpu.VMEM)


def body(
    n,
    tp,
    glu_value,
    glu_gate,
    conv_taps,
    chan_gain,
    chan_shift,
    mix_out_weight,
    moe_input,
    moe_gain,
    expert_ids,
    expert_share,
    expert_gate_weight,
    expert_up_weight,
    expert_down_weight,
):
    tokens, per_token = expert_ids.shape
    width = moe_input.shape[1]
    sh = Shape(n, tp, tokens, per_token, width)
    slab, depth = sh.slab, sh.depth

    positions, channels = glu_value.shape
    taps_count = conv_taps.shape[0]
    margin = -(-(taps_count - 1) // PACK) * PACK
    out_width = mix_out_weight.shape[1]
    hidden_units = expert_gate_weight.shape[2]
    dma = pltpu.SemaphoreType.DMA
    packed = (depth, sh.slots, sh.pack_w)
    mixed, moe_output = pl.pallas_call(
        functools.partial(whole_kernel, sh, taps_count, margin),
        name="mixer_and_experts",
        out_shape=(
            jax.ShapeDtypeStruct((positions, out_width), BF16),
            jax.ShapeDtypeStruct((tokens, width), BF16),
        ),
        in_specs=[ANY] * 13,
        out_specs=(VMEM, VMEM),
        scratch_shapes=[
            pltpu.VMEM((depth, tokens, width), BF16),
            pltpu.VMEM((depth, sh.table_rows, sh.slots), F32),
            pltpu.VMEM(packed, BF16),
            pltpu.VMEM(packed, BF16),
            pltpu.VMEM((sh.count, width), BF16),
            pltpu.VMEM((sh.count, hidden_units), BF16),
            pltpu.VMEM((sh.count, width), BF16),
            pltpu.VMEM(packed, BF16),
            pltpu.VMEM(packed, BF16),
            pltpu.VMEM((depth + 1, tokens, width), BF16),
            pltpu.VMEM((depth, tokens, width), BF16),
            pltpu.VMEM((depth, tokens, width), F32),
            pltpu.VMEM((width, hidden_units), BF16),
            pltpu.VMEM((width, hidden_units), BF16),
            pltpu.VMEM((hidden_units, width), BF16),
            pltpu.VMEM((channels, out_width), BF16),
            pltpu.VMEM((positions, channels), BF16),
            pltpu.VMEM((positions, channels), BF16),
            pltpu.VMEM((margin, channels), BF16),
            pltpu.VMEM((margin, channels), BF16),
            pltpu.VMEM((channels // LANES, margin + positions // depth, LANES), F32),
            pltpu.VMEM((positions // depth, channels), F32),
            pltpu.VMEM((positions, channels), BF16),
            dma((depth, CUT + 1)),
            dma((depth, CUT + 1)),
            dma((depth, CUT + 1)),
            dma((depth, CUT, slab)),
            dma((depth, CUT, slab)),
            dma((depth, CUT, slab)),
            dma((depth, CUT, slab)),
            dma((depth, HOP)),
            dma((depth + 1, HOP)),
            dma((2,)),
            dma((2,)),
            dma((tp, FEED)),
            dma((tp, FEED)),
            dma((tp, FEED)),
            dma((tp, FEED)),
            dma((13,)),
            pltpu.VMEM((tokens, width), BF16),
            pltpu.VMEM((1, width), F32),
            pltpu.VMEM((per_token, tokens), jnp.int32),
            pltpu.VMEM((per_token, tokens), F32),
            pltpu.VMEM((taps_count, channels), F32),
            pltpu.VMEM((1, channels), F32),
            pltpu.VMEM((1, channels), F32),
        ],
        compiler_params=pltpu.CompilerParams(
            collective_id=0, has_side_effects=True, vmem_limit_bytes=67043328
        ),
    )(
        moe_input,
        moe_gain.reshape(1, width),
        expert_ids.T,
        expert_share.T,
        glu_value,
        glu_gate,
        conv_taps,
        chan_gain.reshape(1, channels),
        chan_shift.reshape(1, channels),
        mix_out_weight,
        expert_gate_weight,
        expert_up_weight,
        expert_down_weight,
    )
    return (mixed, moe_output)


def solution(mesh):
    tp = mesh.shape["tp"]
    n = mesh.shape["ep"] * tp
    both = P(("ep", "tp"), None)
    weights = P(("ep", "tp"), None, None)
    placed = (
        both, both, P(), P(), P(), P("tp", None), both, P(), both, both, weights, weights, weights
    )
    return jax.shard_map(
        functools.partial(body, n, tp),
        mesh=mesh,
        in_specs=placed,
        out_specs=(both, both),
        check_vma=False,
    )
```

```python
import functools

import jax
import jax.numpy as jnp
from jax import lax
from jax.experimental import pallas as pl
from jax.experimental.pallas import tpu as pltpu
from jax.sharding import PartitionSpec as P

CLAMP_LIMIT = 7.0
GLU_SLOPE = 1.702
LANES = 128
PACK = 16
CUT = 2
HOP = 8
KINDS = 4
FEED = 2
MESH = pl.DeviceIdType.MESH
F32 = jnp.float32
BF16 = jnp.bfloat16


def place(flat, tp):
    return (flat // tp, flat % tp)


def rows_of(index, size):
    return pl.ds(pl.multiple_of(index * size, size), size)


def visit_order(depth):
    table = []
    for z in range(depth):
        near = sorted(range(depth), key=lambda other: (abs(other - z), other))
        table.append(near)
    return table


def drain_order(depth):
    table = []
    for z in range(depth):
        upward = [(z + k, z + k) for k in range(1, depth - z)] if z > 0 else []
        downward = (
            [(depth - 1 - z + k, z - k) for k in range(1, z + 1)] if z < depth - 1 else []
        )
        events = [target for _, target in sorted(upward + downward)]
        table.append(events + [-1] * (depth - len(events)))
    return table


def looked_up(table, z, slot):
    picked = 0
    for a, row in enumerate(table):
        for b, entry in enumerate(row):
            picked = picked + jnp.where((z == a) & (slot == b), entry, 0)
    return picked


def remote(src, dst, ssem, rsem, flat, tp):
    return pltpu.make_async_remote_copy(
        src_ref=src,
        dst_ref=dst,
        send_sem=ssem,
        recv_sem=rsem,
        device_id=place(flat, tp),
        device_id_type=MESH,
    )


def greet(n, tp, slab, me, with_next):
    barrier = pltpu.get_barrier_semaphore()
    z, s = me // slab, me % slab
    depth = n // slab

    def hail(flat):
        pl.semaphore_signal(barrier, inc=1, device_id=place(flat, tp), device_id_type=MESH)

    @pl.loop(1, slab)
    def _(k):
        hail(z * slab + (s + k) % slab)

    edges = [(z < depth - 1, slab), (z > 0, -slab)]
    if with_next:
        edges.append(((s == slab - 1) & (z < depth - 1), 1))
        edges.append(((s == 0) & (z > 0), -1))
    total = slab - 1
    for there, step in edges:

        @pl.when(there)
        def _():
            hail(me + step)

        total = total + jnp.where(there, 1, 0)
    return total


class Shape:
    def __init__(self, n, tp, tokens, per_token, width):
        slab = tp * max(1, tp // 2)
        while n % slab:
            slab //= 2
        self.n, self.tp, self.slab, self.depth = n, tp, slab, n // slab
        self.tokens, self.width = tokens, width
        copies = tokens * per_token
        capacity = max(2, 5 * copies // (4 * n))
        self.has_main = capacity >= PACK
        spare = 1
        while spare < capacity - PACK or (capacity < PACK and spare < capacity):
            spare *= 2
        self.spare = spare
        self.bits = spare.bit_length() - 1
        self.cuts = PACK // spare
        self.base = PACK if self.has_main else 0
        self.w = width // CUT
        self.main_w = self.w if self.has_main else 0
        self.piece = self.w // self.cuts
        self.block_w = self.main_w + self.piece
        self.pack_w = CUT * self.block_w
        self.slots = slab * PACK
        self.first = self.slots if self.has_main else 0
        self.count = self.first + slab * spare
        self.table_rows = -(-self.depth * KINDS // 8) * 8


def prepare(sh, features_ref, gain, id_rows, share_rows, normed, table):
    n, tokens = sh.n, sh.tokens
    features = features_ref[...].astype(F32)
    scale = lax.rsqrt(jnp.mean(features * features, axis=-1, keepdims=True) + 1e-06)
    normed[...] = (features * scale * gain[...]).astype(BF16)

    def upright(rows):
        rows = rows[...].astype(F32)
        blank = jnp.zeros((8 - rows.shape[0] % 8, tokens), F32)
        return jnp.transpose(jnp.concatenate([rows, blank], axis=0))

    ids = upright(id_rows).astype(jnp.int32)
    share = upright(share_rows)
    expert = lax.broadcasted_iota(jnp.int32, (tokens, n), 1)
    hits = [(ids[:, k : k + 1] == expert).astype(F32) for k in range(id_rows.shape[0])]
    named = hits[0]
    for hit in hits[1:]:
        named = named + hit
    below = (
        lax.broadcasted_iota(jnp.int32, (tokens, tokens), 0)
        > lax.broadcasted_iota(jnp.int32, (tokens, tokens), 1)
    )
    before = jnp.dot(
        below.astype(F32).astype(BF16), named.astype(BF16), preferred_element_type=F32
    )
    number = lax.broadcasted_iota(jnp.int32, (tokens, sh.slots), 0).astype(F32) + 1.0
    lane = lax.broadcasted_iota(jnp.int32, (tokens, sh.slots), 1)
    main_lane = lane
    spare_lane = lane // PACK * sh.spare + lane % sh.spare
    codes = []
    for k, hit in enumerate(hits):
        chosen = ids[:, k : k + 1]
        rank = jnp.sum(before * hit, axis=1, keepdims=True).astype(jnp.int32)
        main_code = jnp.where(rank < sh.base, chosen * PACK + rank, -1)
        spare_code = jnp.where(rank >= sh.base, chosen * sh.spare + rank - sh.base, -1)
        codes.append((main_code, spare_code, share[:, k : k + 1]))
    table[...] = jnp.zeros_like(table)
    for z in range(sh.depth):
        for kind, lanes, start in (
            (0, main_lane, z * sh.slots),
            (1, spare_lane, z * sh.slab * sh.spare),
        ):
            names = jnp.zeros((tokens, sh.slots), F32)
            shares = jnp.zeros((tokens, sh.slots), F32)
            for code in codes:
                hit = code[kind] - start == lanes
                names = names + jnp.where(hit, number, 0.0)
                shares = shares + jnp.where(hit, code[2], 0.0)
            row = z * KINDS + 2 * kind
            table[row : row + 1, :] = jnp.sum(names, axis=0, keepdims=True)
            table[row + 1 : row + 2, :] = jnp.sum(shares, axis=0, keepdims=True)


def whole_kernel(
    sh,
    taps_count,
    margin,
    moe,
    moe_gain,
    id_rows,
    share_rows,
    value_all,
    gate_all,
    taps,
    gain,
    shift,
    weight,
    wg,
    wu,
    wd,
    mixed,
    moe_out,
    held,
    tabs,
    packs,
    takes,
    data,
    hidden,
    total,
    reply,
    back,
    come,
    away,
    parts,
    wg_v,
    wu_v,
    wd_v,
    weight_v,
    mixed_v,
    mix_s,
    value,
    gate,
    halo_v,
    halo_g,
    glu,
    conv,
    act,
    z_r,
    up_s,
    down_s,
    slab_s,
    slab_r,
    back_s,
    back_r,
    line_s,
    line_r,
    halo_s,
    halo_r,
    weight_s,
    weight_r,
    cross_s,
    cross_r,
    feed_s,
    feed_r,
    load_s,
    moe_v,
    moe_gain_v,
    id_v,
    share_v,
    taps_v,
    gain_v,
    shift_v,
):
    n, tp, slab, depth = sh.n, sh.tp, sh.slab, sh.depth
    e = lax.axis_index("ep")
    t = lax.axis_index("tp")
    me = e * tp + t
    z, s = me // slab, me % slab
    positions, channels = value.shape
    blocks = channels // LANES
    shard = weight.shape[0]
    order = visit_order(depth)
    late = drain_order(depth)

    loads = [
        pltpu.make_async_copy(value_all, value, load_s.at[0]),
        pltpu.make_async_copy(gate_all, gate, load_s.at[1]),
        pltpu.make_async_copy(wg.at[0], wg_v, load_s.at[2]),
        pltpu.make_async_copy(wu.at[0], wu_v, load_s.at[3]),
        pltpu.make_async_copy(wd.at[0], wd_v, load_s.at[4]),
        pltpu.make_async_copy(weight, weight_v.at[rows_of(t, shard)], load_s.at[5]),
    ]
    small = [
        pltpu.make_async_copy(here, there, load_s.at[6 + at])
        for at, (here, there) in enumerate(
            (
                (moe, moe_v),
                (moe_gain, moe_gain_v),
                (id_rows, id_v),
                (share_rows, share_v),
                (taps, taps_v),
                (gain, gain_v),
                (shift, shift_v),
            )
        )
    ]
    for load in small + loads:
        load.start()

    def line_copy(part, src, up):
        if part < CUT:
            cols = slice(part * sh.w, (part + 1) * sh.w)
            there = held.at[src, :, cols]
            here = there
        else:
            there = tabs.at[src]
            here = there
        sems = up_s if up else down_s
        return remote(
            here, there, sems.at[src, part], z_r.at[src, part], me + (slab if up else -slab), tp
        )

    def halo_copy(which, dest):
        src, dst = ((value_all, halo_v), (gate_all, halo_g))[which]
        return remote(
            src.at[pl.ds(positions - margin, margin)],
            dst,
            halo_s.at[which],
            halo_r.at[which],
            dest,
            tp,
        )

    sibling = t + 1 - 2 * (t % 2)
    across = slab // tp
    halves = 2 if across % 2 == 0 else 1
    x = (me // tp) % across
    mine = x % halves
    partner = e + 1 - 2 * (x % 2)
    chunk = shard // (halves * FEED)

    def weight_rows(owner, half, c):
        start = owner * shard + (half * FEED + c) * chunk
        return weight_v.at[pl.ds(pl.multiple_of(start, chunk), chunk)]

    def weight_far(k, owner, c):
        start = pl.multiple_of((mine * FEED + c) * chunk, chunk)
        return remote(
            weight.at[pl.ds(start, chunk)],
            weight_rows(owner, mine, c),
            weight_s.at[k, c],
            weight_r.at[k, c],
            e * tp + (t + k) % tp,
            tp,
        )

    def weight_relay(k, owner, c):
        here = weight_rows(owner, mine, c)
        return remote(
            here, here, weight_s.at[k + 1, c], weight_r.at[k + 1, c], e * tp + sibling, tp
        )

    def weight_cross(k, owner, half, c):
        here = weight_rows(owner, half, c)
        return remote(here, here, cross_s.at[k, c], cross_r.at[k, c], partner * tp + t, tp)

    def cross_relay(k, owner, c):
        here = weight_rows(owner, 1 - mine, c)
        return remote(here, here, cross_s.at[k + 1, c], cross_r.at[k + 1, c], e * tp + sibling, tp)

    def weight_own(owner):
        return remote(
            weight,
            weight_v.at[rows_of(owner, shard)],
            weight_s.at[1, 0],
            weight_r.at[1, 0],
            e * tp + sibling,
            tp,
        )

    fed = depth >= 3
    at_end = ((z == 0) | (z == depth - 1)) if fed else z < 0
    inner = jnp.logical_not(at_end)

    def weight_line(k, owner, up):
        here = weight_v.at[rows_of(owner, shard)]
        flat = me + (slab if up else -slab)
        return remote(here, here, feed_s.at[k + (tp if up else 0)], feed_r.at[k], flat, tp)

    def line_relay(k, owner):
        here = weight_v.at[rows_of(owner, shard)]
        return remote(here, here, feed_s.at[k + 1], feed_r.at[k + 1], e * tp + sibling, tp)

    def far_owner(base, k):
        return (base + tp - k) % tp

    def block_copy(slot, h, k, sender, owner):
        cols = slice(h * sh.block_w, (h + 1) * sh.block_w)
        return remote(
            packs.at[slot, rows_of((s + k) % slab, PACK), cols],
            takes.at[slot, rows_of(sender, PACK), cols],
            slab_s.at[slot, h, k],
            slab_r.at[slot, h, k],
            z * slab + owner,
            tp,
        )

    def back_copy(slot, h, k, owner, dest):
        cols = slice(h * sh.block_w, (h + 1) * sh.block_w)
        return remote(
            reply.at[slot, rows_of((s + k) % slab, PACK), cols],
            back.at[slot, rows_of(owner, PACK), cols],
            back_s.at[slot, h, k],
            back_r.at[slot, h, k],
            z * slab + dest,
            tp,
        )

    hop_w = sh.width // HOP
    fold = HOP // CUT

    def chain_copy(p, target, index, up):
        cols = slice(p * hop_w, (p + 1) * hop_w)
        return remote(
            away.at[target, :, cols],
            come.at[index, :, cols],
            line_s.at[target, p],
            line_r.at[index, p],
            me + (slab if up else -slab),
            tp,
        )

    expected = greet(n, tp, slab, me, True)
    for load in small:
        load.wait()
    prepare(sh, moe_v, moe_gain_v, id_v, share_v, held.at[z], tabs.at[z])
    pl.semaphore_wait(pltpu.get_barrier_semaphore(), expected)

    for part in (CUT, *range(CUT)):

        @pl.when(z < depth - 1)
        def _():
            line_copy(part, z, True).start()

        @pl.when(z > 0)
        def _():
            line_copy(part, z, False).start()

    @pl.when(me < n - 1)
    def _():
        for which in range(2):
            halo_copy(which, me + 1).start()

    weight_own(t).start()

    def arrive(k, part):
        for src, there, onward, up in (
            (z - k, z >= k, z < depth - 1, True),
            (z + k, z + k < depth, z > 0, False),
        ):

            @pl.when(there)
            def _():
                line_copy(part, src, up).wait_recv()

            @pl.when(there & onward)
            def _():
                line_copy(part, src, up).start()

    def pack_rows(slot, h, src):
        cols = h * sh.w
        token = lax.broadcasted_iota(jnp.int32, (sh.tokens, sh.slots), 0).astype(F32) + 1.0
        lane = lax.broadcasted_iota(jnp.int32, (sh.tokens, sh.slots), 1)
        at = h * sh.block_w

        def gathered(mask, lo, size):
            return lax.dot_general(
                mask.astype(F32).astype(BF16),
                held[src, :, lo : lo + size],
                (((0,), (0,)), ((), ())),
                preferred_element_type=F32,
            )

        if sh.has_main:
            named = tabs[src, pl.ds(z * KINDS, 1), :]
            packs[slot, :, at : at + sh.w] = gathered(named == token, cols, sh.w).astype(BF16)
        spare_named = tabs[src, pl.ds(z * KINDS + 2, 1), :]
        hit = spare_named == token
        part = (lane >> sh.bits) & (sh.cuts - 1)
        folded = jnp.zeros((sh.slots, sh.piece), F32)
        for q in range(sh.cuts):
            folded = folded + gathered(hit & (part == q), cols + q * sh.piece, sh.piece)
        packs[slot, :, at + sh.main_w : at + sh.block_w] = folded.astype(BF16)

    def home(shape, dim, q):
        row = lax.broadcasted_iota(jnp.int32, shape, dim)
        slot = lax.broadcasted_iota(jnp.int32, shape, 1 - dim)
        where = (row >> sh.bits) * PACK + (row & (sh.spare - 1)) + q * sh.spare
        return (where == slot).astype(F32).astype(BF16)

    spare_rows = slab * sh.spare
    hidden_units = wg_v.shape[1]
    block = min(256, hidden_units)

    def experts(slot):
        for h in range(CUT):
            at = h * sh.block_w
            if sh.has_main:
                data[0 : sh.slots, h * sh.w : (h + 1) * sh.w] = takes[slot, :, at : at + sh.w]
            rest = takes[slot, :, at + sh.main_w : at + sh.block_w]
            for q in range(sh.cuts):
                lo = h * sh.w + q * sh.piece
                data[sh.first : sh.count, lo : lo + sh.piece] = jnp.dot(
                    home((spare_rows, sh.slots), 0, q), rest, preferred_element_type=F32
                ).astype(BF16)

        for f in range(hidden_units // block):
            cols = slice(f * block, (f + 1) * block)
            pre_gate = jnp.dot(data[...], wg_v[:, cols], preferred_element_type=F32)
            pre_up = jnp.dot(data[...], wu_v[:, cols], preferred_element_type=F32)
            gated = jnp.minimum(pre_gate, CLAMP_LIMIT)
            lifted = jnp.clip(pre_up, -CLAMP_LIMIT, CLAMP_LIMIT) + 1.0
            hidden[:, cols] = (lifted * gated * jax.nn.sigmoid(GLU_SLOPE * gated)).astype(BF16)

        step = min(512, sh.width)
        for f in range(sh.width // step):
            cols = slice(f * step, (f + 1) * step)
            total[:, cols] = jnp.dot(
                hidden[...], wd_v[:, cols], preferred_element_type=F32
            ).astype(BF16)

        for h in range(CUT):
            at = h * sh.block_w
            if sh.has_main:
                reply[slot, :, at : at + sh.w] = total[0 : sh.slots, h * sh.w : (h + 1) * sh.w]
            folded = jnp.zeros((sh.slots, sh.piece), F32)
            for q in range(sh.cuts):
                lo = h * sh.w + q * sh.piece
                folded = folded + jnp.dot(
                    home((sh.slots, spare_rows), 1, q),
                    total[sh.first : sh.count, lo : lo + sh.piece],
                    preferred_element_type=F32,
                )
            reply[slot, :, at + sh.main_w : at + sh.block_w] = folded.astype(BF16)

    part_rows = 64
    norm_rows = 32
    lead = margin - (taps_count - 1)
    tile = positions // depth

    def conv_tile(c):
        top = c * tile
        here = rows_of(c, tile)

        @pl.when(c > 0)
        def _():
            for b in range(blocks):
                glu[b, 0:margin, :] = glu[b, tile : tile + margin, :]

        for b in range(blocks):
            cols = slice(b * LANES, (b + 1) * LANES)
            glu[b, margin : margin + tile, :] = value[here, cols].astype(F32) * jax.nn.sigmoid(
                gate[here, cols].astype(F32)
            )

        @pl.loop(0, tile // part_rows)
        def _(r):
            base = r * part_rows
            for b in range(blocks):
                cols = slice(b * LANES, (b + 1) * LANES)
                summed = jnp.zeros((part_rows, LANES), F32)
                for j in range(taps_count):
                    summed = (
                        summed
                        + taps_v[j : j + 1, cols] * glu[b, pl.ds(base + lead + j, part_rows), :]
                    )
                conv[rows_of(r, part_rows), cols] = summed

        @pl.loop(0, tile // norm_rows)
        def _(r):
            rows = conv[rows_of(r, norm_rows), :]
            center = jnp.mean(rows, axis=-1, keepdims=True)
            rows = rows - center
            spread = jnp.mean(rows * rows, axis=-1, keepdims=True)
            normed = rows * lax.rsqrt(spread + 1e-05) * gain_v[...] + shift_v[...]
            there = pl.ds(pl.multiple_of(top + r * norm_rows, norm_rows), norm_rows)
            act[there, :] = (normed * jax.nn.sigmoid(normed)).astype(BF16)

    def weights_of(source, kind):
        token = lax.broadcasted_iota(jnp.int32, (sh.tokens, sh.slots), 0).astype(F32) + 1.0
        named = tabs[source, pl.ds(z * KINDS + kind, 1), :]
        share = tabs[source, pl.ds(z * KINDS + kind + 1, 1), :]
        full = jnp.where(named == token, share, 0.0)
        high = full.astype(BF16)
        low = (full - high.astype(F32)).astype(BF16)
        return high, low

    def weigh(high, low, rows):
        return jnp.dot(high, rows, preferred_element_type=F32) + jnp.dot(
            low, rows, preferred_element_type=F32
        )

    def pass_on(p, target):
        @pl.when(target > z)
        def _():
            chain_copy(p, target, target, True).start()

        @pl.when(target < z)
        def _():
            index = jnp.where(target == z - 1, depth, target)
            chain_copy(p, target, index, False).start()

    def combine(slot):
        target = looked_up(order, z, slot)
        begins = ((z == 0) & (target > 0)) | ((z == depth - 1) & (target < z))
        lane = lax.broadcasted_iota(jnp.int32, (sh.tokens, sh.slots), 1)
        part = (lane >> sh.bits) & (sh.cuts - 1)
        for h in range(CUT):

            @pl.loop(1, slab)
            def _(k):
                back_copy(slot, h, k, (s + slab - k) % slab, s).wait_recv()

            at = h * sh.block_w
            cols = slice(h * sh.w, (h + 1) * sh.w)
            spare_high, spare_low = weights_of(target, 2)
            rest = back[slot, :, at + sh.main_w : at + sh.block_w]
            zero = jnp.zeros_like(spare_high)
            for q in range(sh.cuts):
                lo = h * sh.w + q * sh.piece
                parts[target, :, lo : lo + sh.piece] = weigh(
                    jnp.where(part == q, spare_high, zero),
                    jnp.where(part == q, spare_low, zero),
                    rest,
                )
            if sh.has_main:
                high, low = weights_of(target, 0)
                parts[target, :, cols] += weigh(high, low, back[slot, :, at : at + sh.w])

            @pl.when(begins)
            def _():
                away[target, :, cols] = parts[target, :, cols].astype(BF16)
                for f in range(fold):
                    pass_on(h * fold + f, target)

    out_w = weight_v.shape[1]
    out_step = min(512, out_w)
    mix_rows = positions // (2 * depth)

    def mixed_copy(c):
        here = rows_of(c, mix_rows)
        return pltpu.make_async_copy(mixed_v.at[here], mixed.at[here], mix_s.at[c])

    def mix(c):
        for f in range(out_w // out_step):
            cols = slice(f * out_step, (f + 1) * out_step)
            mixed_v[rows_of(c, mix_rows), cols] = jnp.dot(
                act[rows_of(c, mix_rows), :], weight_v[:, cols], preferred_element_type=F32
            ).astype(BF16)
        mixed_copy(c).start()

    def dispatch(slot, h):
        pack_rows(slot, h, looked_up(order, z, slot))

        @pl.loop(1, slab)
        def _(k):
            block_copy(slot, h, k, s, (s + k) % slab).start()

        cols = slice(h * sh.block_w, (h + 1) * sh.block_w)
        takes[slot, rows_of(s, PACK), cols] = packs[slot, rows_of(s, PACK), cols]

    def send_back(slot):
        for h in range(CUT):

            @pl.loop(1, slab)
            def _(k):
                back_copy(slot, h, k, s, (s + k) % slab).start()

        back[slot, rows_of(s, PACK), :] = reply[slot, rows_of(s, PACK), :]

    last = CUT - 1

    @pl.loop(0, depth + 3)
    def _(i):
        @pl.when(i == depth + 2)
        def _():
            @pl.loop(0, depth)
            def _(k):
                target = looked_up(late, z, k)

                @pl.when(target >= 0)
                def _():
                    for p in range(HOP):
                        cols = slice(p * hop_w, (p + 1) * hop_w)
                        chain_copy(p, target, target, True).wait_recv()
                        away[target, :, cols] = (
                            parts[target, :, cols] + come[target, :, cols].astype(F32)
                        ).astype(BF16)
                        pass_on(p, target)

        @pl.when(i > 2)
        def _():
            combine((i - 2) % depth)

        @pl.when((i > 0) & (i < depth))
        def _():
            arrive(i, last)

        @pl.when(i < depth)
        def _():
            for h in range(last):

                @pl.when(i == 0)
                def _():
                    dispatch(i, h)

            dispatch(i, last)

        for k in range(2, tp, 2):

            @pl.when(inner & (i < FEED))
            def _():
                weight_far(k, t, i).start()

            @pl.when(inner & (i > 0) & (i <= FEED))
            def _():
                weight_far(k, far_owner(t, k), i - 1).wait_recv()
                weight_relay(k, far_owner(t, k), i - 1).start()
                if halves == 2:
                    weight_cross(k, far_owner(t, k), mine, i - 1).start()

            if halves == 2:

                @pl.when(inner & (i > 1) & (i <= FEED + 1))
                def _():
                    weight_cross(k, far_owner(t, k), 1 - mine, i - 2).wait_recv()
                    cross_relay(k, far_owner(t, k), i - 2).start()

            if fed:

                @pl.when((i == FEED + 1) & (z == 1))
                def _():
                    weight_line(k, far_owner(t, k), False).start()

                @pl.when((i == FEED + 1) & (z == depth - 2))
                def _():
                    weight_line(k, far_owner(t, k), True).start()

                @pl.when((i == depth + 1) & at_end)
                def _():
                    weight_line(k, far_owner(t, k), False).wait_recv()
                    line_relay(k, far_owner(t, k)).start()

        @pl.when(i == 0)
        def _():
            loads[0].wait()
            loads[1].wait()

            @pl.when(me > 0)
            def _():
                for which in range(2):
                    halo_copy(which, me - 1).wait_recv()
                for b in range(blocks):
                    cols = slice(b * LANES, (b + 1) * LANES)
                    glu[b, 0:margin, :] = halo_v[:, cols].astype(F32) * jax.nn.sigmoid(
                        halo_g[:, cols].astype(F32)
                    )

            @pl.when(me == 0)
            def _():
                for b in range(blocks):
                    glu[b, 0:margin, :] = jnp.zeros((margin, LANES), F32)

        @pl.when(i < depth)
        def _():
            conv_tile(i)

        @pl.when(i < depth - 1)
        def _():
            arrive(i + 1, CUT)
            for h in range(last):
                arrive(i + 1, h)
                dispatch(i + 1, h)

        @pl.when(i == 0)
        def _():
            for load in loads[2:]:
                load.wait()

        @pl.when(i < depth)
        def _():
            for h in range(CUT):

                @pl.loop(1, slab)
                def _(k):
                    block_copy(i, h, k, (s + slab - k) % slab, s).wait_recv()

            experts(i)

        @pl.when((i > 0) & (i <= depth))
        def _():
            send_back(i % depth)

        @pl.when((inner & (i == depth)) | (at_end & (i == depth + 2)))
        def _():
            weight_own(sibling).wait_recv()
            for k in range(2, tp, 2):

                @pl.when(inner)
                def _():
                    for c in range(FEED):
                        weight_relay(k, far_owner(sibling, k), c).wait_recv()
                        if halves == 2:
                            cross_relay(k, far_owner(sibling, k), c).wait_recv()

                if fed:

                    @pl.when(at_end)
                    def _():
                        line_relay(k, far_owner(sibling, k)).wait_recv()

            @pl.loop(0, 2 * depth)
            def _(c):
                mix(c)

    for p in range(HOP):
        cols = slice(p * hop_w, (p + 1) * hop_w)

        @pl.when(z > 0)
        def _():
            chain_copy(p, z, z, True).wait_recv()
            parts[z, :, cols] += come[z, :, cols].astype(F32)

        @pl.when(z < depth - 1)
        def _():
            chain_copy(p, z, depth, True).wait_recv()
            parts[z, :, cols] += come[depth, :, cols].astype(F32)

        moe_out[:, cols] = parts[z, :, cols].astype(BF16)

    @pl.when(me < n - 1)
    def _():
        for which in range(2):
            halo_copy(which, me + 1).wait_send()

    weight_own(t).wait_send()

    @pl.loop(0, 2 * depth)
    def _(c):
        mixed_copy(c).wait()

    for k in range(2, tp, 2):

        @pl.when(inner)
        def _():
            for c in range(FEED):
                weight_far(k, t, c).wait_send()
                weight_relay(k, far_owner(t, k), c).wait_send()
                if halves == 2:
                    weight_cross(k, far_owner(t, k), mine, c).wait_send()
                    cross_relay(k, far_owner(t, k), c).wait_send()

        if fed:

            @pl.when(at_end)
            def _():
                line_relay(k, far_owner(t, k)).wait_send()

            @pl.when(z == 1)
            def _():
                weight_line(k, far_owner(t, k), False).wait_send()

            @pl.when(z == depth - 2)
            def _():
                weight_line(k, far_owner(t, k), True).wait_send()

    @pl.loop(0, depth)
    def _(c):
        for part in range(CUT + 1):

            @pl.when((z < depth - 1) & (c <= z))
            def _():
                line_copy(part, c, True).wait_send()

            @pl.when((z > 0) & (c >= z))
            def _():
                line_copy(part, c, False).wait_send()

        for h in range(CUT):

            @pl.loop(1, slab)
            def _(k):
                block_copy(c, h, k, s, (s + k) % slab).wait_send()
                back_copy(c, h, k, s, (s + k) % slab).wait_send()

        @pl.when(c != z)
        def _():
            for p in range(HOP):
                chain_copy(p, c, c, True).wait_send()


ANY = pl.BlockSpec(memory_space=pl.ANY)
VMEM = pl.BlockSpec(memory_space=pltpu.VMEM)


def body(
    n,
    tp,
    glu_value,
    glu_gate,
    conv_taps,
    chan_gain,
    chan_shift,
    mix_out_weight,
    moe_input,
    moe_gain,
    expert_ids,
    expert_share,
    expert_gate_weight,
    expert_up_weight,
    expert_down_weight,
):
    tokens, per_token = expert_ids.shape
    width = moe_input.shape[1]
    sh = Shape(n, tp, tokens, per_token, width)
    slab, depth = sh.slab, sh.depth

    positions, channels = glu_value.shape
    taps_count = conv_taps.shape[0]
    margin = -(-(taps_count - 1) // PACK) * PACK
    out_width = mix_out_weight.shape[1]
    hidden_units = expert_gate_weight.shape[2]
    dma = pltpu.SemaphoreType.DMA
    packed = (depth, sh.slots, sh.pack_w)
    mixed, moe_output = pl.pallas_call(
        functools.partial(whole_kernel, sh, taps_count, margin),
        name="mixer_and_experts",
        out_shape=(
            jax.ShapeDtypeStruct((positions, out_width), BF16),
            jax.ShapeDtypeStruct((tokens, width), BF16),
        ),
        in_specs=[ANY] * 13,
        out_specs=(ANY, VMEM),
        scratch_shapes=[
            pltpu.VMEM((depth, tokens, width), BF16),
            pltpu.VMEM((depth, sh.table_rows, sh.slots), F32),
            pltpu.VMEM(packed, BF16),
            pltpu.VMEM(packed, BF16),
            pltpu.VMEM((sh.count, width), BF16),
            pltpu.VMEM((sh.count, hidden_units), BF16),
            pltpu.VMEM((sh.count, width), BF16),
            pltpu.VMEM(packed, BF16),
            pltpu.VMEM(packed, BF16),
            pltpu.VMEM((depth + 1, tokens, width), BF16),
            pltpu.VMEM((depth, tokens, width), BF16),
            pltpu.VMEM((depth, tokens, width), F32),
            pltpu.VMEM((width, hidden_units), BF16),
            pltpu.VMEM((width, hidden_units), BF16),
            pltpu.VMEM((hidden_units, width), BF16),
            pltpu.VMEM((channels, out_width), BF16),
            pltpu.VMEM((positions, out_width), BF16),
            dma((2 * depth,)),
            pltpu.VMEM((positions, channels), BF16),
            pltpu.VMEM((positions, channels), BF16),
            pltpu.VMEM((margin, channels), BF16),
            pltpu.VMEM((margin, channels), BF16),
            pltpu.VMEM((channels // LANES, margin + positions // depth, LANES), F32),
            pltpu.VMEM((positions // depth, channels), F32),
            pltpu.VMEM((positions, channels), BF16),
            dma((depth, CUT + 1)),
            dma((depth, CUT + 1)),
            dma((depth, CUT + 1)),
            dma((depth, CUT, slab)),
            dma((depth, CUT, slab)),
            dma((depth, CUT, slab)),
            dma((depth, CUT, slab)),
            dma((depth, HOP)),
            dma((depth + 1, HOP)),
            dma((2,)),
            dma((2,)),
            dma((tp, FEED)),
            dma((tp, FEED)),
            dma((tp, FEED)),
            dma((tp, FEED)),
            dma((2 * tp,)),
            dma((tp,)),
            dma((13,)),
            pltpu.VMEM((tokens, width), BF16),
            pltpu.VMEM((1, width), F32),
            pltpu.VMEM((per_token, tokens), jnp.int32),
            pltpu.VMEM((per_token, tokens), F32),
            pltpu.VMEM((taps_count, channels), F32),
            pltpu.VMEM((1, channels), F32),
            pltpu.VMEM((1, channels), F32),
        ],
        compiler_params=pltpu.CompilerParams(
            collective_id=0, has_side_effects=True, vmem_limit_bytes=67043328
        ),
    )(
        moe_input,
        moe_gain.reshape(1, width),
        expert_ids.T,
        expert_share.T,
        glu_value,
        glu_gate,
        conv_taps,
        chan_gain.reshape(1, channels),
        chan_shift.reshape(1, channels),
        mix_out_weight,
        expert_gate_weight,
        expert_up_weight,
        expert_down_weight,
    )
    return (mixed, moe_output)


def solution(mesh):
    tp = mesh.shape["tp"]
    n = mesh.shape["ep"] * tp
    both = P(("ep", "tp"), None)
    weights = P(("ep", "tp"), None, None)
    placed = (
        both, both, P(), P(), P(), P("tp", None), both, P(), both, both, weights, weights, weights
    )
    return jax.shard_map(
        functools.partial(body, n, tp),
        mesh=mesh,
        in_specs=placed,
        out_specs=(both, both),
        check_vma=False,
    )
```
